32 devices in a mesh: sp: 8 (over z, x), tp: 4 (over y, core).
Axes of the slice: x: 2, y: 2, z: 4, core: 2. Of those that a mesh axis runs over, the one named last changes fastest.
Arguments:
- stream: bfloat16 [1024, 2048], P('sp'), may hold values from -15 to 15
- cotangent: bfloat16 [1024, 2048], P('sp'), may hold values from -6 to 6
- route_ids: int32 [1024, 2], P('sp'), may hold values from 0 to 7, all different within a row; in each aligned block of 128 rows (0 to 127, 128 to 255, ...) at most 64 rows name the same one
- route_weights: float32 [1024, 2], P('sp'), may hold values from 0.1 to 0.9
- w_gate: bfloat16 [8, 2048, 2048], P('sp', None, 'tp'), may hold values from -0.125 to 0.125
- w_up: bfloat16 [8, 2048, 2048], P('sp', None, 'tp'), may hold values from -0.125 to 0.125
- w_down: bfloat16 [8, 2048, 2048], P('sp', 'tp'), may hold values from -0.125 to 0.125
- out_proj: bfloat16 [2048, 512], P(None, 'tp'), may hold values from -0.25 to 0.25
- mixed: bfloat16 [512, 1024], P('tp', 'sp'), may hold values from -6 to 6
- rec_input: bfloat16 [512, 1024], P('tp', 'sp'), may hold values from -6 to 6
- branch_input: bfloat16 [512, 1024], P('tp', 'sp'), may hold values from -6 to 6
- state_before: float32 [512, 1024], P('tp', 'sp'), may hold values from -6 to 6
- rec_gates: bfloat16 [16, 32, 32], P('tp'), may hold values from -1 to 1
- in_gates: bfloat16 [16, 32, 32], P('tp'), may hold values from -1 to 1
- decay_param: float32 [512], P('tp'), may hold values from 4.4 to 11
- decay_shift: float32 [512, 1024], P('tp', 'sp'), may hold values from -1.4 to -1e-05
Outputs:
- grad_gate: bfloat16 [8, 2048, 2048], P('sp', None, 'tp')
- grad_up: bfloat16 [8, 2048, 2048], P('sp', None, 'tp')
- grad_down: bfloat16 [8, 2048, 2048], P('sp', 'tp')
- grad_proj: float32 [2048, 512], P('sp', 'tp')
- grad_rec: float32 [512, 1024], P('tp', 'sp')
- grad_branch: float32 [512, 1024], P('tp', 'sp')
The draws below stay inside these ranges and needn't reach their ends.
Inputs may be any that keep to these rules, and one draw needn't show every extreme that they name: `route_ids`: each row names 2 different experts; the rows of one device name no expert more than 64 times, a bound that some block reaches on some device.
All inputs are finite; a program needn't handle non-finite values.
Results may differ from the reference program's by a relative error of at most 0.03.
Values may be sent and summed in bfloat16 or wider, within the bound.
A program may use at most 64 MiB of HBM per device.

```python
import math
import jax
import jax.numpy as jnp
import numpy as np
from jax import lax

D = 2048
F = 2048
W = 512
HD = 32
TOP_K = 2
TOK_DEV = 128
HEADS = 16
EXPERTS = 8
SEQUENCE_TOKENS = 1024
CAP = 64
N_SP = 8
N_TP = 4


def draw_decay_param(key, part):
    pick_key, fast_key, slow_key = jax.random.split(jax.random.fold_in(key, 11), 3)
    slow_share = 0.5
    slow_mask = jax.random.uniform(pick_key, (W,), jnp.float32) < slow_share
    fast_value = jax.random.uniform(fast_key, (W,), jnp.float32, 4.4, 5.2)
    slow_value = jax.random.uniform(slow_key, (W,), jnp.float32, 10.0, 11.0)
    return jnp.where(slow_mask, slow_value, fast_value).astype(jnp.float32)


def draw_decay_shift(key, part):
    block_key, location_key, size_key = jax.random.split(jax.random.fold_in(key, 23), 3)
    block_count = SEQUENCE_TOKENS // TOK_DEV
    block_rate = jax.random.uniform(block_key, (W, block_count), jnp.float32, 2e-05, 0.00015)
    stable_baseline = -jnp.repeat(block_rate, TOK_DEV, axis=1)
    spike_locations = jax.random.randint(location_key, (2,), 0, SEQUENCE_TOKENS)
    retained_fraction = jax.random.uniform(size_key, (2, W), jnp.float32, 0.5, 0.8)
    token_position = jnp.arange(SEQUENCE_TOKENS)
    match_count = token_position[None, None, :] == spike_locations[:, None, None]
    spike_events = jnp.sum(jnp.where(match_count, jnp.log(retained_fraction)[:, :, None], 0.0), axis=0)
    return (stable_baseline + spike_events).astype(jnp.float32)


def raised(entries, rng, source, target, parts, factor):
    def block_of(axis_at):
        return (jnp.arange(entries.shape[axis_at]) // (entries.shape[axis_at] // parts)).reshape((-1,) + (1,) * (entries.ndim - 1 - axis_at))

    first = jax.random.permutation(rng, parts)[block_of(target)]
    second = (block_of(target) + parts // 2) % parts
    return jnp.where((block_of(source) == first) | (block_of(source) == second), factor * entries, entries)


def shard_levels(rng, dims, cuts, low, largest):
    level, own = 1.0, jax.random.fold_in(rng, 6)
    for axis_at, blocks in cuts:
        heights = jnp.exp(jax.random.uniform(jax.random.fold_in(own, axis_at), (blocks,), jnp.float32, low / len(cuts), largest / len(cuts)))
        level = level * jnp.repeat(heights, dims[axis_at] // blocks).reshape([-1 if axis == axis_at else 1 for axis in range(len(dims))])
    return level


def shared_out(stream_key, own, number, rows, amount, top, limit, skew):
    order = jax.random.permutation(stream_key, amount)
    packed, ordinary = load_shares(amount, rows * top, limit, skew, True), load_shares(amount, rows * top, limit, skew, False)
    places = jnp.arange(amount)

    def named(tallies, turn):
        used = int((tallies > 0).sum())
        fixed = max(1, used // 4)
        passed = fixed + (places - fixed + turn * (used - fixed)) % max(1, amount - fixed)
        return jnp.zeros((amount,), jnp.int32).at[order[jnp.where(places < fixed, places, passed)]].set(jnp.asarray(tallies, jnp.int32))

    tallies = jnp.where(number % 4 == 0, named(packed, number // 4), named(ordinary, number - number // 4 - 1))
    mixed = jax.random.permutation(jax.random.fold_in(own, 3), amount)
    source_of, sink = mixed[0:amount // 2 * 2:2], mixed[1:amount // 2 * 2:2]
    room = jnp.minimum(tallies[source_of] - 1, limit - tallies[sink]) // 2
    room = jnp.where((source_of == order[0]) | (sink == order[0]) | (tallies[sink] == 0), 0, jnp.maximum(room, 0))
    passed = jax.random.randint(jax.random.fold_in(own, 4), (amount // 2,), 0, 1 << 20) % (room + 1)
    tallies = tallies.at[source_of].add(-passed).at[sink].add(passed)
    members = jnp.searchsorted(jnp.cumsum(tallies), jnp.arange(rows * top), side="right").astype(jnp.int32)
    grid = members.reshape(top, rows).T
    grid = grid[jax.random.permutation(jax.random.fold_in(own, 1), rows)]
    turn = jax.random.randint(jax.random.fold_in(own, 2), (rows, 1), 0, top)
    return jnp.take_along_axis(grid, (jnp.arange(top)[None, :] + turn) % top, axis=1)


def load_shares(amount, total, most, lean, full):
    portions = [(1 << 20) // math.isqrt(rank ** lean) + 1 for rank in range(1, amount + 1)]
    largest = most if full else min(most, max(-(-total // amount), total * portions[0] // sum(portions)))
    least = 1 if total - largest >= amount - 1 else 0
    counts, spare = [largest] + [least] * (amount - 1), total - largest - least * (amount - 1)
    while spare > 0:
        candidates = [i for i in range(1, amount) if counts[i] < largest] or [i for i in range(1, amount) if counts[i] < most]
        mass, budget = sum([portions[i] for i in candidates]), spare
        for i in candidates:
            addition = min(most - counts[i], max(1, budget * portions[i] // mass), spare)
            counts[i] = counts[i] + addition
            spare = spare - addition
    return np.array(counts)


def noise(key, extent, spread, bound, cuts=(), held_as=jnp.bfloat16):
    factor_of = shard_levels(key, extent, cuts, -0.22, 0.18) if cuts else 1.0
    drawn = jax.random.normal(key, extent, jnp.float32) * spread * factor_of
    return jnp.minimum(jnp.maximum(drawn, -bound), bound).astype(held_as)


def noise_with(own_key, shape, width, most, cuts, heavy, kind=jnp.bfloat16):
    array = width * jax.random.normal(own_key, shape, jnp.float32)
    if cuts:
        array = array * shard_levels(own_key, shape, cuts, -0.22, 0.18)
    return jnp.clip(raised(array, jax.random.fold_in(own_key, 3), *heavy), -most, most).astype(kind)


def setup_inputs(seed: int = 0) -> dict:
    arg_keys = jax.random.split(jax.random.key(seed), 17)
    stream = noise(arg_keys[0], (SEQUENCE_TOKENS, D), 2.5, 15.0, ((0, 8),))
    cotangent = noise_with(arg_keys[1], (SEQUENCE_TOKENS, D), 1.0, 6.0, ((0, 8),), (0, 1, 8, 2.0))
    route_ids_keys = jax.random.split(jax.random.fold_in(arg_keys[2], 1), SEQUENCE_TOKENS // TOK_DEV)
    route_ids_turns = jax.random.permutation(jax.random.fold_in(arg_keys[2], 3), SEQUENCE_TOKENS // TOK_DEV)
    route_ids = jax.vmap(lambda own, number: shared_out(jax.random.fold_in(arg_keys[2], 2), own, number, TOK_DEV, EXPERTS, TOP_K, CAP, 1))(route_ids_keys, route_ids_turns).reshape((SEQUENCE_TOKENS, TOP_K))
    route_weights = jnp.clip(0.1 + 0.79999997 * jax.random.uniform(arg_keys[3], (SEQUENCE_TOKENS, TOP_K), jnp.float32) ** shard_levels(arg_keys[3], (SEQUENCE_TOKENS, TOP_K), ((0, 8),), -0.2, 0.2), 0.1, 0.9)
    w_gate = noise(arg_keys[4], (EXPERTS, D, F), D ** -0.5, 0.125, ((0, 8), (2, 4)))
    w_up = noise(arg_keys[5], (EXPERTS, D, F), D ** -0.5, 0.125, ((0, 8), (2, 4)))
    w_down = noise(arg_keys[6], (EXPERTS, F, D), F ** -0.5, 0.125, ((0, 8), (1, 4)))
    out_proj = noise(arg_keys[7], (D, W), W ** -0.5, 0.25, ((1, 4),))
    mixed = noise(arg_keys[8], (W, SEQUENCE_TOKENS), 1.0, 6.0, ((0, 4), (1, 8)))
    rec_input = noise(arg_keys[9], (W, SEQUENCE_TOKENS), 1.0, 6.0, ((0, 4), (1, 8)))
    branch_input = noise(arg_keys[10], (W, SEQUENCE_TOKENS), 1.0, 6.0, ((0, 4), (1, 8)))
    state_before = noise(arg_keys[11], (W, SEQUENCE_TOKENS), 1.0, 6.0, ((0, 4), (1, 8)), jnp.float32)
    rec_gates = noise(arg_keys[12], (HEADS, HD, HD), HD ** -0.5, 1.0, ((0, 4),))
    in_gates = noise(arg_keys[13], (HEADS, HD, HD), HD ** -0.5, 1.0, ((0, 4),))
    decay_param = draw_decay_param(jax.random.fold_in(arg_keys[16], 71), 0)
    decay_shift = draw_decay_shift(jax.random.fold_in(arg_keys[16], 71), 0)
    return {"stream": stream, "cotangent": cotangent, "route_ids": route_ids, "route_weights": route_weights, "w_gate": w_gate, "w_up": w_up, "w_down": w_down, "out_proj": out_proj, "mixed": mixed, "rec_input": rec_input, "branch_input": branch_input, "state_before": state_before, "rec_gates": rec_gates, "in_gates": in_gates, "decay_param": decay_param, "decay_shift": decay_shift}


RATE_SCALE = 8.0
CLAMP_LIMIT = 7.0
GLU_ALPHA = 1.702

def expert_act(gate_pre, up_pre):
    glu_part = jnp.minimum(gate_pre, CLAMP_LIMIT)
    lin_part = jnp.clip(up_pre, -CLAMP_LIMIT, CLAMP_LIMIT)
    return glu_part * jax.nn.sigmoid(GLU_ALPHA * glu_part) * (lin_part + 1.0)

def reverse_step(later_elem, earlier_elem):
    return (later_elem[0] * earlier_elem[0], earlier_elem[1] + earlier_elem[0] * later_elem[1])

def reference(stream, cotangent, route_ids, route_weights, w_gate, w_up, w_down, out_proj, mixed, rec_input, branch_input, state_before, rec_gates, in_gates, decay_param, decay_shift):
    token_count, model_width = cotangent.shape
    top_count = route_ids.shape[1]
    expert_count = w_gate.shape[0]
    hidden = w_gate.shape[2]
    per_device = token_count // N_SP
    capacity = 2 * per_device * top_count // expert_count
    expert_rows = N_SP * capacity
    grouped = route_ids.reshape(N_SP, per_device * top_count)
    onehot = (grouped[:, :, None] == jnp.arange(expert_count, dtype=jnp.int32)[None, None, :]).astype(jnp.int32)
    slot_index = lax.optimization_barrier(jnp.sum((jnp.cumsum(onehot, axis=1) - onehot) * onehot, axis=2))
    device_ids = jnp.arange(N_SP, dtype=jnp.int32)[:, None]
    target = (grouped * expert_rows + device_ids * capacity + slot_index).reshape(-1).astype(jnp.int32)
    scaled = (route_weights[:, :, None] * cotangent[:, None, :].astype(jnp.float32)).astype(jnp.bfloat16)
    scaled = scaled.reshape(-1, model_width)
    copies = jnp.broadcast_to(stream[:, None, :], (token_count, top_count, model_width)).reshape(-1, model_width)
    empty_rows = jnp.zeros((expert_count * expert_rows, model_width), jnp.bfloat16)
    grad_rows = empty_rows.at[target].set(scaled).reshape(expert_count, expert_rows, model_width)
    token_rows = empty_rows.at[target].set(copies).reshape(expert_count, expert_rows, model_width)
    group_width = hidden // N_TP

    def one_expert(expert_item):
        grads_one, tokens_one, gate_one, up_one, down_one = expert_item
        gate_pre = jnp.dot(tokens_one, gate_one, preferred_element_type=jnp.float32)
        up_pre = jnp.dot(tokens_one, up_one, preferred_element_type=jnp.float32)
        act_val, act_vjp = jax.vjp(expert_act, gate_pre, up_pre)
        act_low = act_val.astype(jnp.bfloat16)
        d_act = jnp.dot(grads_one, down_one.T, preferred_element_type=jnp.float32)
        d_gate, d_up = act_vjp(d_act)
        d_gate = d_gate.astype(jnp.bfloat16)
        d_up = d_up.astype(jnp.bfloat16)
        g_gate = jnp.dot(tokens_one.T, d_gate, preferred_element_type=jnp.float32).astype(jnp.bfloat16)
        g_up = jnp.dot(tokens_one.T, d_up, preferred_element_type=jnp.float32).astype(jnp.bfloat16)
        g_down = jnp.dot(act_low.T, grads_one, preferred_element_type=jnp.float32).astype(jnp.bfloat16)
        gate_terms = jnp.einsum('rjf,djf->jrd', d_gate.astype(jnp.float32).reshape(expert_rows, N_TP, group_width), gate_one.astype(jnp.float32).reshape(model_width, N_TP, group_width))
        up_terms = jnp.einsum('rjf,djf->jrd', d_up.astype(jnp.float32).reshape(expert_rows, N_TP, group_width), up_one.astype(jnp.float32).reshape(model_width, N_TP, group_width))
        rounded = lax.optimization_barrier((gate_terms + up_terms).astype(jnp.bfloat16))
        summed = lax.optimization_barrier(jnp.sum(rounded.astype(jnp.float32), axis=0)).astype(jnp.bfloat16)
        return (g_gate, g_up, g_down, summed)
    grad_gate, grad_up, grad_down, slot_grads = lax.map(one_expert, (grad_rows, token_rows, w_gate, w_up, w_down))
    per_pair = slot_grads.reshape(-1, model_width)[target].astype(jnp.float32).reshape(token_count, top_count, model_width)
    stream_low = (cotangent.astype(jnp.float32) + lax.optimization_barrier(jnp.sum(per_pair, axis=1))).astype(jnp.bfloat16)
    d_mixed = lax.dot_general(out_proj, stream_low, (((0,), (1,)), ((), ())), preferred_element_type=jnp.float32)
    grad_proj = lax.dot_general(stream_low, mixed, (((0,), (1,)), ((), ())), preferred_element_type=jnp.float32)
    channels, positions = rec_input.shape
    gate_heads = rec_gates.shape[0]
    head_dim = rec_gates.shape[1]
    rec_value = rec_input.astype(jnp.float32)
    rec_heads = rec_value.reshape(gate_heads, head_dim, positions)
    rec_pre = jnp.einsum('hij,hit->hjt', rec_gates.astype(jnp.float32), rec_heads).reshape(channels, positions)
    in_pre = jnp.einsum('hij,hit->hjt', in_gates.astype(jnp.float32), rec_heads).reshape(channels, positions)
    rec_gate = jax.nn.sigmoid(rec_pre)
    in_gate = jax.nn.sigmoid(in_pre)
    soft_plus = jax.nn.softplus(-decay_param)[:, None]
    log_decay = -RATE_SCALE * rec_gate * soft_plus + decay_shift
    decay_rate = jnp.exp(log_decay)
    at_start = (jnp.arange(positions) == 0)[None, :]
    raw_mult = jnp.sqrt(-jnp.expm1(2.0 * log_decay))
    multiplier = jnp.where(at_start, 1.0, raw_mult)
    state_now = decay_rate * state_before + multiplier * in_gate * rec_value
    gelu_val, gelu_vjp = jax.vjp(jax.nn.gelu, branch_input.astype(jnp.float32))
    grad_branch = gelu_vjp(d_mixed * state_now)[0]
    d_state = d_mixed * gelu_val
    next_decay = jnp.concatenate([decay_rate[:, 1:], jnp.zeros((channels, 1), jnp.float32)], axis=1)
    adjoint = lax.associative_scan(reverse_step, (next_decay, d_state), reverse=True, axis=1)[1]
    mult_term = adjoint * in_gate * rec_value * decay_rate * decay_rate / raw_mult
    d_log = adjoint * state_before * decay_rate - jnp.where(at_start, 0.0, mult_term)
    d_rec_pre = (d_log * -RATE_SCALE * soft_plus * rec_gate * (1.0 - rec_gate)).astype(jnp.bfloat16)
    d_in_pre = (adjoint * multiplier * rec_value * in_gate * (1.0 - in_gate)).astype(jnp.bfloat16)
    d_rec_pre, d_in_pre = lax.optimization_barrier((d_rec_pre, d_in_pre))
    back_rec = jnp.einsum('hij,hjt->hit', rec_gates.astype(jnp.float32), d_rec_pre.astype(jnp.float32).reshape(gate_heads, head_dim, positions))
    back_in = jnp.einsum('hij,hjt->hit', in_gates.astype(jnp.float32), d_in_pre.astype(jnp.float32).reshape(gate_heads, head_dim, positions))
    grad_rec = adjoint * multiplier * in_gate + (back_rec + back_in).reshape(channels, positions)
    return (grad_gate, grad_up, grad_down, grad_proj, grad_rec, grad_branch)
```

```python
import functools

import jax
import jax.numpy as jnp
from jax import lax
from jax.experimental import pallas as pl
from jax.experimental.pallas import tpu as pltpu
from jax.sharding import PartitionSpec as P

RATE_SCALE = 8.0
CLAMP_LIMIT = 7.0
GLU_ALPHA = 1.702
CORES = 2
MESH = pl.DeviceIdType.MESH
VMEM_LIMIT = 60 * 1024 * 1024
GELU_A = 0.7978845608028654
GELU_B = 0.044715
BF = jnp.bfloat16
F32 = jnp.float32


def aligned(value, size):
    return pl.multiple_of(value * size, size)


def part(index, size):
    return pl.ds(aligned(index, size), size)


def remote(src, dst, send_sem, recv_sem, device):
    return pltpu.make_async_remote_copy(
        src_ref=src,
        dst_ref=dst,
        send_sem=send_sem,
        recv_sem=recv_sem,
        device_id=device,
        device_id_type=MESH,
    )


def dot(a, b, da=1, db=0):
    return lax.dot_general(a, b, (((da,), (db,)), ((), ())), preferred_element_type=F32)


def minus_expm1(x):
    series = x * (1.0 + x * (0.5 + x * (1 / 6 + x * (1 / 24 + x * (1 / 120 + x * (1 / 720))))))
    return jnp.where(x > -0.25, -series, 1.0 - jnp.exp(x))


def softplus(v):
    u = jnp.exp(-jnp.abs(v))
    series = u * (1.0 - u * (0.5 - u * (1 / 3 - u * (0.25 - u * (0.2 - u * (1 / 6))))))
    return jnp.maximum(v, 0.0) + jnp.where(u < 0.06, series, jnp.log(1.0 + u))


def sigmoid(x):
    return 1.0 / (1.0 + jnp.exp(-x))


class Place:
    def __init__(self, n_sp, n_tp):
        self.n, self.nt, self.ny = n_sp, n_tp, n_tp // CORES
        self.s, self.t = lax.axis_index("sp"), lax.axis_index("tp")
        self.y, self.c = self.t // CORES, lax.rem(self.t, CORES)
        self.partner = (self.s, self.y * CORES + 1 - self.c)
        quarter = n_sp // 4
        mid = lax.rem(self.s // quarter + self.s // (2 * quarter), 2)
        self.far = (2 * quarter + quarter * mid, 2 * quarter + quarter * (1 - mid))

    def mirror(self, i):
        found, bit = 0, 1
        while bit < self.n:
            found = found + lax.rem(self.s // bit + i // bit, 2) * bit
            bit *= 2
        return found

    def y_peer(self, j):
        return lax.rem(self.y + j, self.ny)

    def y_source(self, j):
        return lax.rem(self.y + self.ny - j, self.ny)

    def tp_of(self, y, c):
        return y * CORES + c

    def q(self, j, same=True):
        return self.tp_of(self.y_source(j), self.c if same else 1 - self.c)

    def y_dev(self, j):
        return (self.s, self.tp_of(self.y_peer(j), self.c))

    def dev(self, i, j):
        return (self.mirror(i), self.tp_of(self.y_peer(j), self.c))


def fused_kernel(n, nt, head_dim, *refs):
    (
        stream, cot, ids, rw, wg_h, wu_h, wd_h, op_h, mixed, rec_in, branch, before, rgate, igate,
        dparam, dshift,
        o_gate, o_up, o_down, o_proj, o_rec, o_branch,
        wg, wu, wd, opf, sc, pos, land, land2, land_t, src, inb, msrc, mb, act, dg, du, wgp, wup,
        q, qin, qsum, ret, ag, au, gp, gin, gsum, yin, gy, xin, gx, zin, st_gate, st_up, st_down,
        level, coef, link, links, mixed_t, dm0, adj0, base,
        w_sem, s1, r1, sy, ry, sx, rx, sm, rm, smy, rmy, smx, rmx, soy, roy, sox, rox,
        sq, rq, sr, rr, sk, rk, sg, rg, sgy, rgy, sgx, rgx, sgz, rgz, o_sem,
    ) = refs
    at = Place(n, nt)
    ny = at.ny
    tok, width = cot.shape
    rows = land.shape[0] // n
    cols = width // nt
    wl, hidden = opf.shape[2], wg.shape[1]
    top = ids.shape[1]
    blk = width // n
    half = n // 2
    quarter = n // 4
    groups = [list(range(nt))] if wl % 128 == 0 else [[b] for b in range(nt)]
    ftile = min(256, hidden)

    def cat(ref, sl, group):
        parts = [ref[b, sl, :] for b in group]
        return parts[0] if len(parts) == 1 else jnp.concatenate(parts, axis=1)

    def spread(value, group, put):
        for at_b, b in enumerate(group):
            put(b, value[:, at_b * wl : (at_b + 1) * wl])

    def loop(lo, hi, body):
        def step(i, carry):
            body(i)
            return carry

        lax.fori_loop(lo, hi, step, 0)

    barrier = pltpu.get_barrier_semaphore()

    def greet(device):
        pl.semaphore_signal(barrier, inc=1, device_id=device, device_id_type=MESH)

    def greet_all(i):
        for j in range(ny):
            greet(at.dev(i, j))

    loop(1, n, greet_all)
    for j in range(1, ny):
        greet(at.y_dev(j))
    greet(at.partner)

    weights = [
        pltpu.make_async_copy(op_h, opf.at[at.t], w_sem.at[0]),
        pltpu.make_async_copy(wg_h, wg, w_sem.at[1]),
        pltpu.make_async_copy(wu_h, wu, w_sem.at[2]),
        pltpu.make_async_copy(wd_h, wd, w_sem.at[3]),
    ]
    for copy in weights:
        copy.start()

    lane = lax.broadcasted_iota(jnp.int32, (tok, tok), 1)
    sub = lax.broadcasted_iota(jnp.int32, (tok, tok), 0)
    eye = lane == sub
    eye_low = jnp.where(eye, 1.0, 0.0).astype(BF)
    tri = jnp.where(sub < lane, 1.0, 0.0).astype(BF)
    expert_at = lax.broadcasted_iota(jnp.int32, (n, tok), 0).astype(F32)
    named = []
    for k in range(top):
        column = ids[:, k : k + 1].astype(F32)
        row = jnp.sum(jnp.where(eye, column, 0.0), axis=0, keepdims=True)
        named.append(expert_at == row)
    count = functools.reduce(jnp.add, [jnp.where(m, 1.0, 0.0) for m in named])
    earlier = dot(count.astype(BF), tri)
    for k in range(top):
        pos[k] = jnp.where(named[k], earlier, -1.0)
    slot = lax.broadcasted_iota(jnp.int32, (rows, tok), 0).astype(F32)

    def lands(i):
        e = at.mirror(i)
        hits = [jnp.where(pos[k, pl.ds(e, 1), :] == slot, 1.0, 0.0) for k in range(top)]
        land[part(i, rows), :] = functools.reduce(jnp.add, hits).astype(BF)
        for k in range(top):
            land2[part(i, rows), k * tok : (k + 1) * tok] = hits[k].astype(BF)

    loop(0, n, lands)

    def scale(b):
        sl = part(b, cols)
        value = cot[:, sl].astype(F32)
        for k in range(top):
            sc[k * tok : (k + 1) * tok, sl] = (rw[:, k : k + 1] * value).astype(BF)

    loop(0, nt, scale)

    def to_slots(lo, hi, tp, put):
        sl, rs = part(tp, cols), slice(lo * rows, hi * rows)
        put(rs, slice(0, cols), dot(land[rs, :], stream[:, sl]).astype(BF))
        put(rs, slice(cols, 2 * cols), dot(land2[rs, :], sc[:, sl]).astype(BF))

    def put_src(j):
        def put(rs, cs, value):
            src[j, rs, cs] = value

        return put

    for j in range(ny):
        to_slots(1, half, at.q(j), put_src(j))

    def first(i, j):
        return remote(
            src.at[j, part(i, rows), :],
            inb.at[at.q(j), part(i, rows), :],
            s1.at[i, j],
            r1.at[i, j],
            (at.mirror(i), at.t),
        )

    def along_y(i, j, outgoing):
        spot = inb.at[at.t if outgoing else at.q(j), part(i, rows), :]
        return remote(spot, spot, sy.at[i, j], ry.at[i, j], at.y_dev(j))

    def across(i, j, outgoing):
        spot = inb.at[at.q(j, outgoing), part(i, rows), :]
        return remote(spot, spot, sx.at[i, j], rx.at[i, j], at.partner)

    def op_y(j, outgoing):
        spot = opf.at[at.t if outgoing else at.q(j)]
        return remote(spot, spot, soy.at[j], roy.at[j], at.y_dev(j))

    def op_x(j, outgoing):
        spot = opf.at[at.q(j, outgoing)]
        return remote(spot, spot, sox.at[j], rox.at[j], at.partner)

    def m_first(i):
        return remote(
            msrc.at[part(i, rows), :],
            mb.at[at.t, part(i, rows), :],
            sm.at[i],
            rm.at[i],
            (at.mirror(i), at.t),
        )

    def m_y(j, outgoing):
        spot = mb.at[at.t if outgoing else at.q(j)]
        return remote(spot, spot, smy.at[j], rmy.at[j], at.y_dev(j))

    def m_x(j, outgoing):
        spot = mb.at[at.q(j, outgoing)]
        return remote(spot, spot, smx.at[j], rmx.at[j], at.partner)

    weights[0].wait()
    pl.semaphore_wait(barrier, (n - 1) * ny + ny - 1 + 1)
    for j in range(1, ny):
        op_y(j, True).start()
    op_x(0, True).start()

    def send_near(i):
        for j in range(ny):
            first(i, j).start()

    loop(1, half, send_near)
    to_slots(half, n, at.t, put_src(0))
    msrc[...] = dot(land[...], mixed[...], 1, 1).astype(BF)

    def own_slots(tp):
        def put(rs, cs, value):
            inb[tp, rs, cs] = value

        to_slots(0, 1, tp, put)

    loop(0, nt, own_slots)
    for far in at.far:
        loop(0, quarter, lambda k: first(far + k, 0).start())
    mb[at.t, 0:rows, :] = msrc[0:rows, :]
    loop(1, half, lambda i: m_first(i).start())
    for far in at.far:
        loop(0, quarter, lambda k: m_first(far + k).start())

    lane_w = lax.broadcasted_iota(jnp.int32, (wl, wl), 1)
    sub_w = lax.broadcasted_iota(jnp.int32, (wl, wl), 0)
    eye_w = lane_w == sub_w

    def to_col(row):
        return jnp.sum(jnp.where(eye_w, row, 0.0), axis=1, keepdims=True)

    def to_row(col):
        return jnp.sum(jnp.where(eye_w, col, 0.0), axis=0, keepdims=True)

    repeat = jnp.where(
        lax.rem(lax.broadcasted_iota(jnp.int32, (head_dim, wl), 1), head_dim)
        == lax.broadcasted_iota(jnp.int32, (head_dim, wl), 0),
        1.0,
        0.0,
    ).astype(BF)
    same_head = lax.div(lane_w, head_dim) == lax.div(sub_w, head_dim)

    def diagonal(ref):
        return jnp.where(same_head, dot(ref[...], repeat), 0.0).astype(BF)

    time_at = lax.broadcasted_iota(jnp.int32, (wl, tok), 1)
    rec = rec_in[...]
    rec_gate = sigmoid(dot(diagonal(rgate), rec, 0, 0))
    in_gate = sigmoid(dot(diagonal(igate), rec, 0, 0))
    rec = rec.astype(F32)
    soft = to_col(softplus(-dparam[...]))
    log_decay = -RATE_SCALE * rec_gate * soft + dshift[...]
    decay = jnp.exp(log_decay)
    at_start = (time_at == 0) & (at.s == 0)
    raw_mult = jnp.sqrt(minus_expm1(2.0 * log_decay))
    multiplier = jnp.where(at_start, 1.0, raw_mult)
    old = before[...]
    state = decay * old + multiplier * in_gate * rec
    x = branch[...].astype(F32)
    th = jnp.tanh(GELU_A * (x + GELU_B * x * x * x))
    gelu = 0.5 * x * (1.0 + th)
    slope = 0.5 * (1.0 + th) + 0.5 * x * (1.0 - th * th) * GELU_A * (1.0 + 3.0 * GELU_B * x * x)
    mult_part = jnp.where(at_start, 0.0, in_gate * rec * decay * decay / raw_mult)
    coef[0] = gelu
    coef[1] = state * slope
    coef[2] = (old * decay - mult_part) * (-RATE_SCALE * soft) * rec_gate * (1.0 - rec_gate)
    coef[3] = multiplier * rec * in_gate * (1.0 - in_gate)
    coef[4] = multiplier * in_gate
    step_decay = jnp.where(time_at == tok - 1, 0.0, pltpu.roll(decay, tok - 1, 1))
    tail = jnp.where(time_at == tok - 1, 1.0, pltpu.roll(decay, tok - 1, 1))
    shift, depth = 1, 0
    while shift < tok:
        level[depth] = step_decay
        step_decay = step_decay * pltpu.roll(step_decay, tok - shift, 1)
        tail = tail * jnp.where(time_at < tok - shift, pltpu.roll(tail, tok - shift, 1), 1.0)
        shift, depth = shift * 2, depth + 1
    coef[5] = tail
    coef[6] = decay
    link[...] = jnp.zeros(link.shape, F32)
    link[0:1, :] = to_row(decay[:, 0:1] * tail[:, 0:1])
    dm0[...] = dot(cot[...], opf[at.t])
    mixed_t[...] = dot(eye_low, mixed[...], 1, 1).astype(BF)
    land_t[...] = dot(eye_low, land[...], 1, 1).astype(BF)

    def own_part(b):
        base[part(b, cols), :] = dot(cot[:, part(b, cols)], mixed_t[...], 0, 0)

    loop(0, nt, own_part)
    for copy in weights[1:]:
        copy.wait()

    def near_in(i):
        for j in range(ny):
            first(i, j).wait_recv()
            across(i, j, True).start()

    def far_in(i):
        first(i, 0).wait_recv()
        for j in range(1, ny):
            along_y(i, j, True).start()
        across(i, 0, True).start()

    def far_pass(i):
        for j in range(1, ny):
            along_y(i, j, False).wait_recv()
            across(i, j, True).start()

    def all_here(i):
        for j in range(ny):
            across(i, j, False).wait_recv()

    def forward(r0, size):
        rs = pl.ds(r0, size)

        def tile(f):
            fs = part(f, ftile)
            gate = up = d_act = 0.0
            for b in range(nt):
                bs = slice(b * cols, (b + 1) * cols)
                tokens, grads = inb[b, rs, 0:cols], inb[b, rs, cols : 2 * cols]
                gate = gate + dot(tokens, wg[bs, fs])
                up = up + dot(tokens, wu[bs, fs])
                d_act = d_act + dot(grads, wd[fs, bs], 1, 1)
            glu = jnp.minimum(gate, CLAMP_LIMIT)
            lin = jnp.clip(up, -CLAMP_LIMIT, CLAMP_LIMIT) + 1.0
            sig = sigmoid(GLU_ALPHA * glu)
            gs = glu * sig
            act[rs, fs] = (gs * lin).astype(BF)
            curve = lin * (sig + GLU_ALPHA * gs * (1.0 - sig))
            dg[rs, fs] = jnp.where(gate > CLAMP_LIMIT, 0.0, d_act * curve).astype(BF)
            du[rs, fs] = jnp.where(jnp.abs(up) > CLAMP_LIMIT, 0.0, d_act * gs).astype(BF)

        loop(0, hidden // ftile, tile)

    def project(r0, size):
        rs = pl.ds(r0, size)
        for group in groups:
            value = dot(dg[rs, :], cat(wgp, slice(None), group))
            value = value + dot(du[rs, :], cat(wup, slice(None), group))

            def put(b, piece):
                q[b, rs, :] = piece.astype(BF)

            spread(value, group, put)

    def q_core(g, r0, size, j, outgoing):
        yj = at.y_peer(j)
        return remote(
            q.at[at.tp_of(yj, 1 - at.c), pl.ds(r0, size), :],
            qin.at[j, pl.ds(r0, size), :],
            sq.at[g, j],
            rq.at[g, j],
            at.partner,
        )

    def ret_copy(i, j):
        return remote(
            qsum.at[j, part(i, rows), :],
            ret.at[j, part(i, rows), :],
            sr.at[i, j],
            rr.at[i, j],
            at.dev(i, j),
        )

    def q_send(g, r0, size):
        for j in range(ny):
            q_core(g, r0, size, j, True).start()

    def q_reduce(g, r0, size):
        rs = pl.ds(r0, size)
        for j in range(ny):
            q_core(g, r0, size, j, False).wait_recv()
            mine = q[at.tp_of(at.y_peer(j), at.c), rs, :].astype(F32)
            qsum[j, rs, :] = (mine + qin[j, rs, :].astype(F32)).astype(BF)

    def ret_send(i):
        for j in range(ny):
            ret_copy(i, j).start()

    loop(1, half, near_in)
    for far in at.far[:1]:
        loop(0, quarter, lambda k: far_in(far + k))
    for j in range(1, ny):
        op_y(j, False).wait_recv()
        op_x(j, True).start()
    for far in at.far[:1]:
        loop(0, quarter, lambda k: far_pass(far + k))
    for j in range(ny):
        op_x(j, False).wait_recv()

    def weight_maps(f):
        fs = part(f, ftile)
        for group in groups:
            for ref, out in ((wg, wgp), (wu, wup)):
                value = 0.0
                for b in range(nt):
                    bs = slice(b * cols, (b + 1) * cols)
                    value = value + dot(ref[bs, fs], cat(opf, bs, group), 0, 0)

                def put(b, piece):
                    out[b, fs, :] = piece.astype(BF)

                spread(value, group, put)

    loop(0, hidden // ftile, weight_maps)
    loop(1, half, all_here)
    near_rows = half * rows
    far_rows = quarter * rows
    forward(0, near_rows)
    project(0, near_rows)
    q_send(0, 0, near_rows)
    far_a, far_b = (aligned(far, rows) for far in at.far)
    loop(0, quarter, lambda k: all_here(at.far[0] + k))
    forward(far_a, far_rows)
    project(far_a, far_rows)
    q_send(1, far_a, far_rows)
    q_reduce(0, 0, near_rows)
    loop(0, quarter, lambda k: far_in(at.far[1] + k))
    loop(0, quarter, lambda k: far_pass(at.far[1] + k))
    q_reduce(1, far_a, far_rows)
    loop(0, quarter, lambda k: all_here(at.far[1] + k))
    forward(far_b, far_rows)
    project(far_b, far_rows)
    q_send(2, far_b, far_rows)

    ret[0, 0:rows, :] = qsum[0, 0:rows, :]
    for j in range(1, ny):
        ret_copy(0, j).start()
    loop(1, half, ret_send)
    loop(0, quarter, lambda k: ret_send(at.far[0] + k))

    loop(1, n, lambda i: m_first(i).wait_recv())
    for j in range(1, ny):
        m_y(j, True).start()
    m_x(0, True).start()

    q_reduce(2, far_b, far_rows)
    loop(0, quarter, lambda k: ret_send(at.far[1] + k))

    for j in range(1, ny):
        m_y(j, False).wait_recv()
        m_x(j, True).start()
    for j in range(ny):
        m_x(j, False).wait_recv()

    def inner(f):
        fs = part(f, ftile)
        for group in groups:
            right = cat(mb, slice(None), group)
            for ref, out in ((dg, ag), (du, au)):
                value = dot(ref[:, fs], right, 0, 0)

                def put(b, piece):
                    out[b, fs, :] = piece.astype(BF)

                spread(value, group, put)

    loop(0, hidden // ftile, inner)

    def g_core(k, j):
        return remote(
            gp.at[k, at.tp_of(at.y_peer(j), 1 - at.c)],
            gin.at[k, j],
            sg.at[k, j],
            rg.at[k, j],
            at.partner,
        )

    def outer(k):
        ds = part(at.mirror(k), blk)
        own = base[ds, :]
        for group in groups:
            value = dot(wg[ds, :], cat(ag, slice(None), group))
            value = value + dot(wu[ds, :], cat(au, slice(None), group))

            def put(b, piece):
                gp[k, b] = (piece + jnp.where(at.t == b, own, 0.0)).astype(BF)

            spread(value, group, put)
        for j in range(ny):
            g_core(k, j).start()

    def g_y(k, j):
        return remote(gsum.at[k, j], yin.at[k, j], sgy.at[k, j], rgy.at[k, j], at.y_dev(j))

    def g_x(k):
        return remote(gy.at[k], xin.at[k], sgx.at[k], rgx.at[k], (at.mirror(1), at.t))

    def g_z(k):
        return remote(gx.at[k], zin.at[k], sgz.at[k], rgz.at[k], (at.mirror(2 * k), at.t))

    def core_step(k):
        for j in range(ny):
            g_core(k, j).wait_recv()
            mine = gp[k, at.tp_of(at.y_peer(j), at.c)].astype(F32)
            gsum[k, j] = (mine + gin[k, j].astype(F32)).astype(BF)
            if j:
                g_y(k, j).start()

    def y_step(k):
        total = gsum[k, 0].astype(F32)
        for j in range(1, ny):
            g_y(k, j).wait_recv()
            total = total + yin[k, j].astype(F32)
        gy[k] = total.astype(BF)

    def down(i):
        return n - 1 - i

    loop(0, n, lambda i: outer(down(i)))
    loop(0, n, lambda i: core_step(down(i)))

    def wide_tile(d):
        per = cols // min(256, cols)
        size = cols // per
        b, inside = lax.div(d, per), lax.rem(d, per)
        tokens = inb[b, :, part(inside, size)]
        out = part(d, size)
        st_gate[out, :] = dot(tokens, dg[...], 0, 0).astype(BF)
        st_up[out, :] = dot(tokens, du[...], 0, 0).astype(BF)

    loop(0, width // min(256, cols), wide_tile)
    outs = [
        pltpu.make_async_copy(st_gate, o_gate, o_sem.at[0]),
        pltpu.make_async_copy(st_up, o_up, o_sem.at[1]),
        pltpu.make_async_copy(st_down, o_down, o_sem.at[2]),
    ]
    outs[0].start()
    outs[1].start()

    def ret_here(i):
        for j in range(ny):
            ret_copy(i, j).wait_recv()

    for j in range(1, ny):
        ret_copy(0, j).wait_recv()
    loop(1, n, ret_here)
    total = dm0[...]
    for j in range(ny):
        total = total + dot(land_t[...], ret[j])
    d_mixed = total.T
    o_branch[...] = d_mixed * coef[1]
    run = d_mixed * coef[0]
    shift = 1
    for k in range(depth):
        run = run + level[k] * pltpu.roll(run, tok - shift, 1)
        shift *= 2
    adj0[...] = run
    link[1:2, :] = to_row(coef[6][:, 0:1] * run[:, 0:1])

    def link_copy(i):
        return remote(link, links.at[i], sk.at[i], rk.at[i], (at.mirror(i), at.t))

    loop(1, n, lambda i: link_copy(i).start())

    loop(0, n, lambda i: y_step(down(i)))
    loop(0, half, lambda k: g_x(2 * (half - 1 - k) + 1).start())

    def down_tile(f):
        fs = part(f, ftile)
        left = act[:, fs]
        for b in range(nt):
            bs = slice(b * cols, (b + 1) * cols)
            st_down[fs, bs] = dot(left, inb[b, :, cols : 2 * cols], 0, 0).astype(BF)

    loop(0, hidden // ftile, down_tile)
    outs[2].start()

    loop(1, n, lambda i: link_copy(i).wait_recv())
    links[0] = link[...]

    def compose(k, carry):
        p = n - 1 - k
        lower = links[at.mirror(p)]
        return jnp.where(p > at.s, lower[0:1] * carry + lower[1:2], carry)

    carried = lax.fori_loop(0, n, compose, jnp.zeros((1, wl), F32))
    adjoint = adj0[...] + coef[5] * to_col(carried)
    d_rec = (adjoint * coef[2]).astype(BF)
    d_in = (adjoint * coef[3]).astype(BF)
    o_rec[...] = adjoint * coef[4] + dot(diagonal(rgate), d_rec) + dot(diagonal(igate), d_in)

    def x_step(i):
        k = half - 1 - i
        g_x(2 * k + 1).wait_recv()
        gx[k] = (gy[2 * k].astype(F32) + xin[2 * k + 1].astype(F32)).astype(BF)

    loop(0, half, x_step)
    loop(0, half - 1, lambda i: g_z(half - 1 - i).start())
    o_proj[...] = gx[0].astype(F32)

    def z_step(i):
        k = i + 1
        g_z(k).wait_recv()
        o_proj[...] += zin[k].astype(F32)

    loop(0, half - 1, z_step)

    def drain(i):
        link_copy(i).wait_send()
        m_first(i).wait_send()
        first(i, 0).wait_send()
        across(i, 0, True).wait_send()
        for j in range(1, ny):
            across(i, j, True).wait_send()

            @pl.when(i < half)
            def _():
                first(i, j).wait_send()

            @pl.when(i >= half)
            def _():
                along_y(i, j, True).wait_send()

        for j in range(ny):
            ret_copy(i, j).wait_send()

    loop(1, n, drain)
    for j in range(1, ny):
        ret_copy(0, j).wait_send()
        op_y(j, True).wait_send()
        m_y(j, True).wait_send()
    for j in range(ny):
        op_x(j, True).wait_send()
        m_x(j, True).wait_send()
        q_core(0, 0, near_rows, j, True).wait_send()
        q_core(1, far_a, far_rows, j, True).wait_send()
        q_core(2, far_b, far_rows, j, True).wait_send()

    def drain_sums(k):
        for j in range(ny):
            g_core(k, j).wait_send()
            if j:
                g_y(k, j).wait_send()

    loop(0, n, drain_sums)
    loop(0, half, lambda k: g_x(2 * k + 1).wait_send())
    loop(1, half, lambda k: g_z(k).wait_send())
    for copy in outs:
        copy.wait()


def fused(args, n, nt):
    (stream, cot, ids, rw, wg, wu, wd, op, mixed, rec_in, branch, before, rgate, igate, dparam, dshift) = args
    tok, width = cot.shape
    top = ids.shape[1]
    local_experts, _, hidden = wg.shape
    assert local_experts == 1
    rows = 2 * tok * top // n
    total, ny, cols, wl, blk, half = n * rows, nt // CORES, width // nt, op.shape[1], width // n, n // 2
    head_dim = rgate.shape[1]
    channels = wl
    dma = pltpu.SemaphoreType.DMA

    def buf(*shape, dtype=BF):
        return pltpu.VMEM(shape, dtype)

    depth = max(1, (tok - 1).bit_length())
    scratch = [
        buf(width, hidden), buf(width, hidden), buf(hidden, width),
        buf(nt, width, wl),
        buf(top * tok, width),
        buf(top, n, tok, dtype=F32),
        buf(total, tok), buf(total, top * tok), buf(tok, total),
        buf(ny, total, 2 * cols), buf(nt, total, 2 * cols),
        buf(total, wl), buf(nt, total, wl),
        buf(total, hidden), buf(total, hidden), buf(total, hidden),
        buf(nt, hidden, wl), buf(nt, hidden, wl),
        buf(nt, total, wl), buf(ny, total, wl), buf(ny, total, wl), buf(ny, total, wl),
        buf(nt, hidden, wl), buf(nt, hidden, wl),
        buf(n, nt, blk, wl), buf(n, ny, blk, wl), buf(n, ny, blk, wl), buf(n, ny, blk, wl),
        buf(n, blk, wl), buf(n, blk, wl), buf(half, blk, wl), buf(half, blk, wl),
        buf(width, hidden), buf(width, hidden), buf(hidden, width),
        buf(depth, wl, tok, dtype=F32), buf(7, wl, tok, dtype=F32),
        buf(8, wl, dtype=F32), buf(n, 8, wl, dtype=F32),
        buf(tok, wl), buf(tok, wl, dtype=F32), buf(wl, tok, dtype=F32), buf(width, wl, dtype=F32),
        dma((4,)),
        dma((n, ny)), dma((n, ny)), dma((n, ny)), dma((n, ny)), dma((n, ny)), dma((n, ny)),
        dma((n,)), dma((n,)), dma((ny,)), dma((ny,)), dma((ny,)), dma((ny,)),
        dma((ny,)), dma((ny,)), dma((ny,)), dma((ny,)),
        dma((3, ny)), dma((3, ny)), dma((n, ny)), dma((n, ny)), dma((n,)), dma((n,)),
        dma((n, ny)), dma((n, ny)), dma((n, ny)), dma((n, ny)),
        dma((n,)), dma((n,)), dma((half,)), dma((half,)), dma((3,)),
    ]
    vm = pl.BlockSpec(memory_space=pltpu.VMEM)
    hb = pl.BlockSpec(memory_space=pl.ANY)
    shape = jax.ShapeDtypeStruct
    return pl.pallas_call(
        functools.partial(fused_kernel, n, nt, head_dim),
        out_shape=(
            shape((width, hidden), BF),
            shape((width, hidden), BF),
            shape((hidden, width), BF),
            shape((blk, wl), F32),
            shape((channels, tok), F32),
            shape((channels, tok), F32),
        ),
        in_specs=[vm] * 4 + [hb] * 4 + [vm] * 8,
        out_specs=[hb] * 3 + [vm] * 3,
        scratch_shapes=scratch,
        compiler_params=pltpu.CompilerParams(
            collective_id=0, has_side_effects=True, vmem_limit_bytes=VMEM_LIMIT
        ),
    )(
        stream, cot, ids, rw, wg[0], wu[0], wd[0], op, mixed, rec_in, branch, before,
        rgate.reshape(-1, head_dim), igate.reshape(-1, head_dim), dparam[None], dshift,
    )


def local(*args):
    n, nt = lax.axis_size("sp"), lax.axis_size("tp")
    gate, up, down, proj, rec, branch = fused(args, n, nt)
    return gate[None], up[None], down[None], proj, rec, branch


def solution(mesh):
    placed = (
        P("sp", None),
        P("sp", None),
        P("sp", None),
        P("sp", None),
        P("sp", None, "tp"),
        P("sp", None, "tp"),
        P("sp", "tp", None),
        P(None, "tp"),
        P("tp", "sp"),
        P("tp", "sp"),
        P("tp", "sp"),
        P("tp", "sp"),
        P("tp", None, None),
        P("tp", None, None),
        P("tp"),
        P("tp", "sp"),
    )
    return jax.shard_map(
        local,
        mesh=mesh,
        in_specs=placed,
        out_specs=(
            P("sp", None, "tp"),
            P("sp", None, "tp"),
            P("sp", "tp", None),
            P("sp", "tp"),
            P("tp", "sp"),
            P("tp", "sp"),
        ),
        check_vma=False,
    )
```

```python
import functools

import jax
import jax.numpy as jnp
from jax import lax
from jax.experimental import pallas as pl
from jax.experimental.pallas import tpu as pltpu
from jax.sharding import PartitionSpec as P

RATE_SCALE = 8.0
CLAMP_LIMIT = 7.0
GLU_ALPHA = 1.702
CORES = 2
MESH = pl.DeviceIdType.MESH
MIB = 1024 * 1024
GELU_A = 0.7978845608028654
GELU_B = 0.044715
BF = jnp.bfloat16
F32 = jnp.float32


def aligned(value, size):
    return pl.multiple_of(value * size, size)


def part(index, size):
    return pl.ds(aligned(index, size), size)


def remote(src, dst, send_sem, recv_sem, device):
    return pltpu.make_async_remote_copy(
        src_ref=src,
        dst_ref=dst,
        send_sem=send_sem,
        recv_sem=recv_sem,
        device_id=device,
        device_id_type=MESH,
    )


def dot(a, b, da=1, db=0):
    return lax.dot_general(a, b, (((da,), (db,)), ((), ())), preferred_element_type=F32)


def minus_expm1(x):
    series = x * (1.0 + x * (0.5 + x * (1 / 6 + x * (1 / 24 + x * (1 / 120 + x * (1 / 720))))))
    return jnp.where(x > -0.25, -series, 1.0 - jnp.exp(x))


def softplus(v):
    u = jnp.exp(-jnp.abs(v))
    series = u * (1.0 - u * (0.5 - u * (1 / 3 - u * (0.25 - u * (0.2 - u * (1 / 6))))))
    return jnp.maximum(v, 0.0) + jnp.where(u < 0.06, series, jnp.log(1.0 + u))


def sigmoid(x):
    return 1.0 / (1.0 + jnp.exp(-x))


class Place:
    def __init__(self, n_sp, n_tp):
        self.n, self.nt, self.ny = n_sp, n_tp, n_tp // CORES
        self.s, self.t = lax.axis_index("sp"), lax.axis_index("tp")
        self.y, self.c = self.t // CORES, lax.rem(self.t, CORES)
        self.partner = (self.s, self.y * CORES + 1 - self.c)
        quarter = n_sp // 4
        self.far = (2 * quarter, 3 * quarter)

    def mirror(self, i):
        found, bit = 0, 1
        while bit < self.n:
            found = found + lax.rem(self.s // bit + i // bit, 2) * bit
            bit *= 2
        return found

    def y_peer(self, j):
        return lax.rem(self.y + j, self.ny)

    def y_source(self, j):
        return lax.rem(self.y + self.ny - j, self.ny)

    def tp_of(self, y, c):
        return y * CORES + c

    def q(self, j, same=True):
        return self.tp_of(self.y_source(j), self.c if same else 1 - self.c)

    def y_dev(self, j):
        return (self.s, self.tp_of(self.y_peer(j), self.c))

    def dev(self, i, j):
        return (self.mirror(i), self.tp_of(self.y_peer(j), self.c))


def fused_kernel(n, nt, head_dim, *refs):
    (
        stream_h, cot_h, ids_h, rw_h, wg_h, wu_h, wd_h, op_h, mixed_h, rec_h, branch_h, before_h,
        rgate_h, igate_h, dparam_h, dshift_h,
        st_gate, st_up, st_down, o_proj, o_rec, o_branch,
        wg, wu, wd, opf, sc, pos, land, land2, land_t, src, inb, msrc, mb, act, dg, du, wgp, wup,
        q, qin, qsum, ret, ag, au, gp, gin, gsum, yin, gy, xin, gx, zin, xin2, mx, yin2,
        level, coef, link, links, mixed_t, dm0, adj0, base,
        stream, cot, ids, rw, mixed, rec_in, branch, before, rgate, igate, dparam, dshift,
        w_sem, s1, r1, sy, ry, sx, rx, sm, rm, smy, rmy, smx, rmx, soy, roy, sox, rox,
        sq, rq, sr, rr, sk, rk, sg, rg, sgy, rgy, sgx, rgx, sgz, rgz, sx2, rx2, sy2, ry2,
    ) = refs
    at = Place(n, nt)
    ny = at.ny
    tok, width = cot_h.shape
    rows = land.shape[0] // n
    cols = width // nt
    wl, hidden = opf.shape[2], wg.shape[1]
    top = ids_h.shape[0]
    blk = width // n
    half = n // 2
    quarter = n // 4
    groups = [list(range(nt))] if wl % 128 == 0 else [[b] for b in range(nt)]
    ftile = min(256, hidden)

    def cat(ref, sl, group):
        parts = [ref[b, sl, :] for b in group]
        return parts[0] if len(parts) == 1 else jnp.concatenate(parts, axis=1)

    def spread(value, group, put):
        for at_b, b in enumerate(group):
            put(b, value[:, at_b * wl : (at_b + 1) * wl])

    def loop(lo, hi, body):
        def step(i, carry):
            body(i)
            return carry

        lax.fori_loop(lo, hi, step, 0)

    pairs = (
        (ids_h, ids), (rw_h, rw), (stream_h, stream), (cot_h, cot), (op_h, opf.at[at.t]),
        (mixed_h, mixed), (rec_h, rec_in), (branch_h, branch), (before_h, before),
        (rgate_h, rgate), (igate_h, igate), (dparam_h, dparam), (dshift_h, dshift),
        (wg_h, wg), (wu_h, wu), (wd_h, wd),
    )
    loads = [pltpu.make_async_copy(a, b, w_sem.at[i]) for i, (a, b) in enumerate(pairs)]

    for copy in loads:
        copy.start()

    barrier = pltpu.get_barrier_semaphore()

    def greet(device):
        pl.semaphore_signal(barrier, inc=1, device_id=device, device_id_type=MESH)

    def greet_all(i):
        for j in range(ny):
            greet(at.dev(i, j))

    loop(1, n, greet_all)
    for j in range(1, ny):
        greet(at.y_dev(j))
    greet(at.partner)


    lane = lax.broadcasted_iota(jnp.int32, (tok, tok), 1)
    sub = lax.broadcasted_iota(jnp.int32, (tok, tok), 0)
    eye = lane == sub
    eye_low = jnp.where(eye, 1.0, 0.0).astype(BF)
    tri = jnp.where(sub < lane, 1.0, 0.0).astype(BF)
    expert_at = lax.broadcasted_iota(jnp.int32, (n, tok), 0).astype(F32)
    named = []
    loads[0].wait()
    loads[1].wait()
    for k in range(top):
        named.append(expert_at == ids[k : k + 1, :].astype(F32))
    count = functools.reduce(jnp.add, [jnp.where(m, 1.0, 0.0) for m in named])
    earlier = dot(count.astype(BF), tri)
    for k in range(top):
        pos[k] = jnp.where(named[k], earlier, -1.0)
    slot = lax.broadcasted_iota(jnp.int32, (rows, tok), 0).astype(F32)

    def lands(i):
        e = at.mirror(i)
        hits = [jnp.where(pos[k, pl.ds(e, 1), :] == slot, 1.0, 0.0) for k in range(top)]
        land[part(i, rows), :] = functools.reduce(jnp.add, hits).astype(BF)
        for k in range(top):
            land2[part(i, rows), k * tok : (k + 1) * tok] = hits[k].astype(BF)

    loop(0, n, lands)

    share = [
        jnp.sum(jnp.where(eye, rw[k : k + 1, :], 0.0), axis=1, keepdims=True) for k in range(top)
    ]

    def scale(b):
        sl = part(b, cols)
        value = cot[:, sl].astype(F32)
        for k in range(top):
            sc[k * tok : (k + 1) * tok, sl] = (share[k] * value).astype(BF)

    loads[2].wait()
    loads[3].wait()
    loop(0, nt, scale)

    def to_slots(lo, hi, tp, put):
        sl, rs = part(tp, cols), slice(lo * rows, hi * rows)
        put(rs, slice(0, cols), dot(land[rs, :], stream[:, sl]).astype(BF))
        put(rs, slice(cols, 2 * cols), dot(land2[rs, :], sc[:, sl]).astype(BF))

    def put_src(j):
        def put(rs, cs, value):
            src[j, rs, cs] = value

        return put

    for j in range(ny):
        to_slots(1, half, at.q(j), put_src(j))

    def first(i, j):
        return remote(
            src.at[j, part(i, rows), :],
            inb.at[at.q(j), part(i, rows), :],
            s1.at[i, j],
            r1.at[i, j],
            (at.mirror(i), at.t),
        )

    def along_y(i, j, outgoing):
        spot = inb.at[at.t if outgoing else at.q(j), part(i, rows), :]
        return remote(spot, spot, sy.at[i, j], ry.at[i, j], at.y_dev(j))

    def across(i, j, outgoing):
        spot = inb.at[at.q(j, outgoing), part(i, rows), :]
        return remote(spot, spot, sx.at[i, j], rx.at[i, j], at.partner)

    def op_y(j, outgoing):
        spot = opf.at[at.t if outgoing else at.q(j)]
        return remote(spot, spot, soy.at[j], roy.at[j], at.y_dev(j))

    def op_x(j, outgoing):
        spot = opf.at[at.q(j, outgoing)]
        return remote(spot, spot, sox.at[j], rox.at[j], at.partner)

    def m_first(i):
        return remote(
            msrc.at[part(i, rows), :],
            mb.at[at.t, part(i, rows), :],
            sm.at[i],
            rm.at[i],
            (at.mirror(i), at.t),
        )

    def m_y(j, outgoing):
        spot = mb.at[at.t if outgoing else at.q(j)]
        return remote(spot, spot, smy.at[j], rmy.at[j], at.y_dev(j))

    def m_x(j, outgoing):
        spot = mb.at[at.q(j, outgoing)]
        return remote(spot, spot, smx.at[j], rmx.at[j], at.partner)

    loads[4].wait()
    loads[5].wait()
    pl.semaphore_wait(barrier, (n - 1) * ny + ny - 1 + 1)
    for j in range(1, ny):
        op_y(j, True).start()
    op_x(0, True).start()

    def send_near(i):
        for j in range(ny):
            first(i, j).start()

    split = half - half // 4
    loop(1, split, send_near)
    to_slots(half, n, at.t, put_src(0))
    msrc[...] = dot(land[...], mixed[...], 1, 1).astype(BF)

    def own_slots(tp):
        def put(rs, cs, value):
            inb[tp, rs, cs] = value

        to_slots(0, 1, tp, put)

    loop(0, nt, own_slots)
    far_1, far_2 = at.far
    loop(far_1, far_2, lambda i: first(i, 0).start())
    mb[at.t, 0:rows, :] = msrc[0:rows, :]

    lane_w = lax.broadcasted_iota(jnp.int32, (wl, wl), 1)
    sub_w = lax.broadcasted_iota(jnp.int32, (wl, wl), 0)
    eye_w = lane_w == sub_w

    def to_col(row):
        return jnp.sum(jnp.where(eye_w, row, 0.0), axis=1, keepdims=True)

    def to_row(col):
        return jnp.sum(jnp.where(eye_w, col, 0.0), axis=0, keepdims=True)

    repeat = jnp.where(
        lax.rem(lax.broadcasted_iota(jnp.int32, (head_dim, wl), 1), head_dim)
        == lax.broadcasted_iota(jnp.int32, (head_dim, wl), 0),
        1.0,
        0.0,
    ).astype(BF)
    same_head = lax.div(lane_w, head_dim) == lax.div(sub_w, head_dim)

    def diagonal(ref):
        return jnp.where(same_head, dot(ref[...], repeat), 0.0).astype(BF)

    for copy in loads[6:13]:
        copy.wait()
    time_at = lax.broadcasted_iota(jnp.int32, (wl, tok), 1)
    rec = rec_in[...]
    rec_gate = sigmoid(dot(diagonal(rgate), rec, 0, 0))
    in_gate = sigmoid(dot(diagonal(igate), rec, 0, 0))
    rec = rec.astype(F32)
    soft = to_col(softplus(-dparam[...]))
    log_decay = -RATE_SCALE * rec_gate * soft + dshift[...]
    decay = jnp.exp(log_decay)
    at_start = (time_at == 0) & (at.s == 0)
    raw_mult = jnp.sqrt(minus_expm1(2.0 * log_decay))
    multiplier = jnp.where(at_start, 1.0, raw_mult)
    old = before[...]
    state = decay * old + multiplier * in_gate * rec
    x = branch[...].astype(F32)
    th = jnp.tanh(GELU_A * (x + GELU_B * x * x * x))
    gelu = 0.5 * x * (1.0 + th)
    slope = 0.5 * (1.0 + th) + 0.5 * x * (1.0 - th * th) * GELU_A * (1.0 + 3.0 * GELU_B * x * x)
    mult_part = jnp.where(at_start, 0.0, in_gate * rec * decay * decay / raw_mult)
    coef[0] = gelu
    coef[1] = state * slope
    coef[2] = (old * decay - mult_part) * (-RATE_SCALE * soft) * rec_gate * (1.0 - rec_gate)
    coef[3] = multiplier * rec * in_gate * (1.0 - in_gate)
    coef[4] = multiplier * in_gate
    step_decay = jnp.where(time_at == tok - 1, 0.0, pltpu.roll(decay, tok - 1, 1))
    tail = jnp.where(time_at == tok - 1, 1.0, pltpu.roll(decay, tok - 1, 1))
    shift, depth = 1, 0
    while shift < tok:
        level[depth] = step_decay
        step_decay = step_decay * pltpu.roll(step_decay, tok - shift, 1)
        tail = tail * jnp.where(time_at < tok - shift, pltpu.roll(tail, tok - shift, 1), 1.0)
        shift, depth = shift * 2, depth + 1
    coef[5] = tail
    coef[6] = decay
    link[...] = jnp.zeros(link.shape, F32)
    link[0:1, :] = to_row(decay[:, 0:1] * tail[:, 0:1])
    dm0[...] = dot(cot[...], opf[at.t])
    mixed_t[...] = dot(eye_low, mixed[...], 1, 1).astype(BF)
    land_t[...] = dot(eye_low, land[...], 1, 1).astype(BF)

    def own_part(b):
        base[part(b, cols), :] = dot(cot[:, part(b, cols)], mixed_t[...], 0, 0)

    loop(0, nt, own_part)
    for copy in loads[13:]:
        copy.wait()

    def near_in(i):
        for j in range(ny):
            first(i, j).wait_recv()
            across(i, j, True).start()

    def far_in(i):
        first(i, 0).wait_recv()
        for j in range(1, ny):
            along_y(i, j, True).start()
        across(i, 0, True).start()

    def far_pass(i):
        for j in range(1, ny):
            along_y(i, j, False).wait_recv()
            across(i, j, True).start()

    def all_here(i):
        for j in range(ny):
            across(i, j, False).wait_recv()

    def forward(r0, size):
        rs = pl.ds(r0, size)

        def tile(f):
            fs = part(f, ftile)
            gate = up = d_act = 0.0
            for b in range(nt):
                bs = slice(b * cols, (b + 1) * cols)
                tokens, grads = inb[b, rs, 0:cols], inb[b, rs, cols : 2 * cols]
                gate = gate + dot(tokens, wg[bs, fs])
                up = up + dot(tokens, wu[bs, fs])
                d_act = d_act + dot(grads, wd[fs, bs], 1, 1)
            glu = jnp.minimum(gate, CLAMP_LIMIT)
            lin = jnp.clip(up, -CLAMP_LIMIT, CLAMP_LIMIT) + 1.0
            sig = sigmoid(GLU_ALPHA * glu)
            gs = glu * sig
            act[rs, fs] = (gs * lin).astype(BF)
            curve = lin * (sig + GLU_ALPHA * gs * (1.0 - sig))
            dg[rs, fs] = jnp.where(gate > CLAMP_LIMIT, 0.0, d_act * curve).astype(BF)
            du[rs, fs] = jnp.where(jnp.abs(up) > CLAMP_LIMIT, 0.0, d_act * gs).astype(BF)

        loop(0, hidden // ftile, tile)

    def project(r0, size):
        rs = pl.ds(r0, size)
        for group in groups:
            value = dot(dg[rs, :], cat(wgp, slice(None), group))
            value = value + dot(du[rs, :], cat(wup, slice(None), group))

            def put(b, piece):
                q[b, rs, :] = piece.astype(BF)

            spread(value, group, put)

    def q_core(g, r0, size, j, outgoing):
        yj = at.y_peer(j)
        return remote(
            q.at[at.tp_of(yj, 1 - at.c), pl.ds(r0, size), :],
            qin.at[j, pl.ds(r0, size), :],
            sq.at[g, j],
            rq.at[g, j],
            at.partner,
        )

    def ret_copy(i, j):
        return remote(
            qsum.at[j, part(i, rows), :],
            ret.at[j, part(i, rows), :],
            sr.at[i, j],
            rr.at[i, j],
            at.dev(i, j),
        )

    def q_send(g, r0, size):
        for j in range(ny):
            q_core(g, r0, size, j, True).start()

    def q_reduce(g, r0, size):
        rs = pl.ds(r0, size)
        for j in range(ny):
            q_core(g, r0, size, j, False).wait_recv()
            mine = q[at.tp_of(at.y_peer(j), at.c), rs, :].astype(F32)
            qsum[j, rs, :] = (mine + qin[j, rs, :].astype(F32)).astype(BF)

    def ret_send(i):
        for j in range(ny):
            ret_copy(i, j).start()

    def weight_maps(f):
        fs = part(f, ftile)
        for group in groups:
            for ref, out in ((wg, wgp), (wu, wup)):
                value = 0.0
                for b in range(nt):
                    bs = slice(b * cols, (b + 1) * cols)
                    value = value + dot(ref[bs, fs], cat(opf, bs, group), 0, 0)

                def put(b, piece):
                    out[b, fs, :] = piece.astype(BF)

                spread(value, group, put)

    near_rows = half * rows
    far_rows = quarter * rows
    far_a, far_b = far_1 * rows, far_2 * rows
    near_in(1)
    loop(far_1, far_2, lambda i: first(i, 0).wait_send())
    loop(split, half, send_near)
    loop(far_2, n, lambda i: first(i, 0).start())
    loop(1, n, lambda i: m_first(i).start())
    loop(2, split, near_in)
    for j in range(1, ny):
        op_y(j, False).wait_recv()
        op_x(j, True).start()
    loop(far_1, far_2, far_in)
    for j in range(ny):
        op_x(j, False).wait_recv()
    loop(0, hidden // ftile, weight_maps)
    loop(far_1, far_2, far_pass)
    loop(split, half, near_in)
    loop(far_2, n, far_in)
    loop(1, half, all_here)
    forward(0, near_rows)
    project(0, near_rows)
    q_send(0, 0, near_rows)
    loop(1, n, lambda i: m_first(i).wait_recv())
    for j in range(1, ny):
        m_y(j, True).start()
    m_x(0, True).start()
    loop(far_1, far_2, all_here)
    forward(far_a, far_rows)
    project(far_a, far_rows)
    q_send(1, far_a, far_rows)
    loop(far_2, n, far_pass)
    q_reduce(0, 0, near_rows)
    q_reduce(1, far_a, far_rows)
    ret[0, 0:rows, :] = qsum[0, 0:rows, :]
    for j in range(1, ny):
        ret_copy(0, j).start()
    loop(1, far_2, ret_send)
    loop(far_2, n, all_here)
    forward(far_b, far_rows)
    project(far_b, far_rows)
    q_send(2, far_b, far_rows)
    for j in range(1, ny):
        m_y(j, False).wait_recv()
        m_x(j, True).start()
    q_reduce(2, far_b, far_rows)
    loop(far_2, n, ret_send)
    for j in range(ny):
        m_x(j, False).wait_recv()

    def inner(f):
        fs = part(f, ftile)
        for group in groups:
            right = cat(mb, slice(None), group)
            for ref, out in ((dg, ag), (du, au)):
                value = dot(ref[:, fs], right, 0, 0)

                def put(b, piece):
                    out[b, fs, :] = piece.astype(BF)

                spread(value, group, put)

    loop(0, hidden // ftile, inner)

    def g_core(k, j):
        return remote(
            gp.at[k, at.tp_of(at.y_peer(j), 1 - at.c)],
            gin.at[k, j],
            sg.at[k, j],
            rg.at[k, j],
            at.partner,
        )

    def outer(k):
        ds = part(at.mirror(k), blk)
        own = base[ds, :]
        for group in groups:
            value = dot(wg[ds, :], cat(ag, slice(None), group))
            value = value + dot(wu[ds, :], cat(au, slice(None), group))

            def put(b, piece):
                gp[k, b] = (piece + jnp.where(at.t == b, own, 0.0)).astype(BF)

            spread(value, group, put)
        for j in range(ny):
            g_core(k, j).start()

    def g_y(k, j):
        return remote(gsum.at[k, j], yin.at[k, j], sgy.at[k, j], rgy.at[k, j], at.y_dev(j))

    def g_x(k):
        return remote(gy.at[k], xin.at[k], sgx.at[k], rgx.at[k], (at.mirror(1), at.t))

    def g_z(k):
        return remote(gx.at[k], zin.at[k], sgz.at[k], rgz.at[k], (at.mirror(2 * k), at.t))

    def g_x2(k, j):
        return remote(
            gsum.at[2 * k + 1, j], xin2.at[k, j], sx2.at[k, j], rx2.at[k, j], (at.mirror(1), at.t)
        )

    def g_y2(k, j):
        return remote(mx.at[k, j], yin2.at[k, j], sy2.at[k, j], ry2.at[k, j], at.y_dev(j))

    cross = half // 2

    def core_step(k, y_first):
        for j in range(ny):
            g_core(k, j).wait_recv()
            mine = gp[k, at.tp_of(at.y_peer(j), at.c)].astype(F32)
            gsum[k, j] = (mine + gin[k, j].astype(F32)).astype(BF)
            if y_first:
                if j:
                    g_y(k, j).start()
            else:

                @pl.when(lax.rem(k, 2) == 1)
                def _():
                    g_x2(lax.div(k, 2), j).start()

    def y_step(k):
        total = gsum[k, 0].astype(F32)
        for j in range(1, ny):
            g_y(k, j).wait_recv()
            total = total + yin[k, j].astype(F32)
        gy[k] = total.astype(BF)

    def y_pair(k):
        y_step(2 * k + 1)
        g_x(2 * k + 1).start()
        y_step(2 * k)

    def x_step(k):
        g_x(2 * k + 1).wait_recv()
        gx[k] = (gy[2 * k].astype(F32) + xin[2 * k + 1].astype(F32)).astype(BF)
        g_z(k).start()

    def x2_step(k):
        for j in range(ny):
            g_x2(k, j).wait_recv()
            both = gsum[2 * k, j].astype(F32) + xin2[k, j].astype(F32)
            mx[k, j] = both.astype(BF)
            if j:
                g_y2(k, j).start()

    def y2_step(k):
        total = mx[k, 0].astype(F32)
        for j in range(1, ny):
            g_y2(k, j).wait_recv()
            total = total + yin2[k, j].astype(F32)
        return total

    def y2_send(k):
        gx[k] = y2_step(k).astype(BF)
        g_z(k).start()

    def wide_tile(d):
        per = cols // min(256, cols)
        size = cols // per
        b, inside = lax.div(d, per), lax.rem(d, per)
        tokens = inb[b, :, part(inside, size)]
        out = part(d, size)
        st_gate[out, :] = dot(tokens, dg[...], 0, 0).astype(BF)
        st_up[out, :] = dot(tokens, du[...], 0, 0).astype(BF)

    def down_tile(f):
        fs = part(f, ftile)
        left = act[:, fs]
        for b in range(nt):
            bs = slice(b * cols, (b + 1) * cols)
            st_down[fs, bs] = dot(left, inb[b, :, cols : 2 * cols], 0, 0).astype(BF)

    outer(n - 1)
    outer(n // 2 - 1)

    def outer_high(i):
        outer(n - 2 - i)
        core_step(n - 1 - i, True)

    def outer_low(i):
        outer(half - 2 - i)
        core_step(half - 1 - i, False)

    def outer_both(i):
        outer_high(i)
        outer_low(i)

    loop(0, half - 1, outer_both)
    core_step(half, True)
    core_step(0, False)

    def tiles(lo, hi):
        count = width // min(256, cols)
        loop(lo * count // 8, hi * count // 8, wide_tile)

    y_pair(half - 1)
    x2_step(cross - 1)
    tiles(0, 2)
    def ret_here(i):
        for j in range(ny):
            ret_copy(i, j).wait_recv()

    for j in range(1, ny):
        ret_copy(0, j).wait_recv()
    loop(1, n, ret_here)
    total = dm0[...]
    for j in range(ny):
        total = total + dot(land_t[...], ret[j])
    d_mixed = total.T
    o_branch[...] = d_mixed * coef[1]
    run = d_mixed * coef[0]
    shift = 1
    for k in range(depth):
        run = run + level[k] * pltpu.roll(run, tok - shift, 1)
        shift *= 2
    adj0[...] = run
    link[1:2, :] = to_row(coef[6][:, 0:1] * run[:, 0:1])

    def link_copy(i):
        return remote(link, links.at[i], sk.at[i], rk.at[i], (at.mirror(i), at.t))

    loop(1, n, lambda i: link_copy(i).start())
    x_step(half - 1)
    for k in range(1, half - cross):
        y_pair(half - 1 - k)
        x2_step(cross - 1 - k)
        y2_send(cross - k)
        tiles(2, 5) if k == 1 else None
        x_step(half - 1 - k)
    tiles(5, 8)
    o_proj[...] = y2_step(0)
    loop(1, n, lambda i: link_copy(i).wait_recv())
    links[0] = link[...]

    def compose(k, carry):
        p = n - 1 - k
        lower = links[at.mirror(p)]
        return jnp.where(p > at.s, lower[0:1] * carry + lower[1:2], carry)

    carried = lax.fori_loop(0, n, compose, jnp.zeros((1, wl), F32))
    adjoint = adj0[...] + coef[5] * to_col(carried)
    d_rec = (adjoint * coef[2]).astype(BF)
    d_in = (adjoint * coef[3]).astype(BF)
    o_rec[...] = adjoint * coef[4] + dot(diagonal(rgate), d_rec) + dot(diagonal(igate), d_in)

    loop(0, hidden // ftile, down_tile)

    def z_step(i):
        k = half - 1 - i
        g_z(k).wait_recv()
        o_proj[...] += zin[k].astype(F32)

    loop(0, half - 1, z_step)

    def drain(i):
        link_copy(i).wait_send()
        m_first(i).wait_send()
        across(i, 0, True).wait_send()
        @pl.when((i < far_1) | (i >= far_2))
        def _():
            first(i, 0).wait_send()

        for j in range(1, ny):
            across(i, j, True).wait_send()

            @pl.when(i < half)
            def _():
                first(i, j).wait_send()

            @pl.when(i >= half)
            def _():
                along_y(i, j, True).wait_send()

        for j in range(ny):
            ret_copy(i, j).wait_send()

    loop(1, n, drain)
    for j in range(1, ny):
        ret_copy(0, j).wait_send()
        op_y(j, True).wait_send()
        m_y(j, True).wait_send()
    for j in range(ny):
        op_x(j, True).wait_send()
        m_x(j, True).wait_send()
        q_core(0, 0, near_rows, j, True).wait_send()
        q_core(1, far_a, far_rows, j, True).wait_send()
        q_core(2, far_b, far_rows, j, True).wait_send()

    def drain_sums(k):
        for j in range(ny):
            g_core(k, j).wait_send()

    loop(0, n, drain_sums)

    def drain_high(k):
        for j in range(1, ny):
            g_y(2 * k, j).wait_send()
            g_y(2 * k + 1, j).wait_send()
        g_x(2 * k + 1).wait_send()

    def drain_low(k):
        for j in range(ny):
            g_x2(k, j).wait_send()
            if j:
                g_y2(k, j).wait_send()

    loop(cross, half, drain_high)
    loop(0, cross, drain_low)
    loop(1, half, lambda k: g_z(k).wait_send())


def fused(args, n, nt):
    (stream, cot, ids, rw, wg, wu, wd, op, mixed, rec_in, branch, before, rgate, igate, dparam, dshift) = args
    tok, width = cot.shape
    top = ids.shape[0]
    local_experts, _, hidden = wg.shape
    assert local_experts == 1
    rows = 2 * tok * top // n
    total, ny, cols, wl, blk, half = n * rows, nt // CORES, width // nt, op.shape[1], width // n, n // 2
    head_dim, cross = rgate.shape[1], half // 2
    channels = wl
    dma = pltpu.SemaphoreType.DMA

    def buf(*shape, dtype=BF):
        return pltpu.VMEM(shape, dtype)

    depth = max(1, (tok - 1).bit_length())
    scratch = [
        buf(width, hidden), buf(width, hidden), buf(hidden, width),
        buf(nt, width, wl),
        buf(top * tok, width),
        buf(top, n, tok, dtype=F32),
        buf(total, tok), buf(total, top * tok), buf(tok, total),
        buf(ny, total, 2 * cols), buf(nt, total, 2 * cols),
        buf(total, wl), buf(nt, total, wl),
        buf(total, hidden), buf(total, hidden), buf(total, hidden),
        buf(nt, hidden, wl), buf(nt, hidden, wl),
        buf(nt, total, wl), buf(ny, total, wl), buf(ny, total, wl), buf(ny, total, wl),
        buf(nt, hidden, wl), buf(nt, hidden, wl),
        buf(n, nt, blk, wl), buf(n, ny, blk, wl), buf(n, ny, blk, wl), buf(n, ny, blk, wl),
        buf(n, blk, wl), buf(n, blk, wl), buf(half, blk, wl), buf(half, blk, wl),
        buf(cross, ny, blk, wl), buf(cross, ny, blk, wl), buf(cross, ny, blk, wl),
        buf(depth, wl, tok, dtype=F32), buf(7, wl, tok, dtype=F32),
        buf(8, wl, dtype=F32), buf(n, 8, wl, dtype=F32),
        buf(tok, wl), buf(tok, wl, dtype=F32), buf(wl, tok, dtype=F32), buf(width, wl, dtype=F32),
        buf(tok, width), buf(tok, width), buf(top, tok, dtype=jnp.int32), buf(top, tok, dtype=F32),
        buf(wl, tok), buf(wl, tok), buf(wl, tok), buf(wl, tok, dtype=F32),
        buf(wl, head_dim), buf(wl, head_dim), buf(1, wl, dtype=F32), buf(wl, tok, dtype=F32),
        dma((16,)),
        dma((n, ny)), dma((n, ny)), dma((n, ny)), dma((n, ny)), dma((n, ny)), dma((n, ny)),
        dma((n,)), dma((n,)), dma((ny,)), dma((ny,)), dma((ny,)), dma((ny,)),
        dma((ny,)), dma((ny,)), dma((ny,)), dma((ny,)),
        dma((3, ny)), dma((3, ny)), dma((n, ny)), dma((n, ny)), dma((n,)), dma((n,)),
        dma((n, ny)), dma((n, ny)), dma((n, ny)), dma((n, ny)),
        dma((n,)), dma((n,)), dma((half,)), dma((half,)),
        dma((cross, ny)), dma((cross, ny)), dma((cross, ny)), dma((cross, ny)),
    ]
    operands = (
        stream, cot, ids, rw, wg[0], wu[0], wd[0], op, mixed, rec_in, branch, before,
        rgate.reshape(-1, head_dim), igate.reshape(-1, head_dim), dparam[None], dshift,
    )
    kept = 6 * width * hidden + 4 * blk * wl + 8 * wl * tok + MIB
    vm = pl.BlockSpec(memory_space=pltpu.VMEM)
    hb = pl.BlockSpec(memory_space=pltpu.HBM)
    shape = pltpu.VMEM
    return pl.pallas_call(
        functools.partial(fused_kernel, n, nt, head_dim),
        out_shape=(
            shape((width, hidden), BF),
            shape((width, hidden), BF),
            shape((hidden, width), BF),
            shape((blk, wl), F32),
            shape((channels, tok), F32),
            shape((channels, tok), F32),
        ),
        in_specs=[hb] * 16,
        out_specs=[vm] * 6,
        scratch_shapes=scratch,
        compiler_params=pltpu.CompilerParams(
            collective_id=0, has_side_effects=True, vmem_limit_bytes=62 * MIB - kept
        ),
    )(*[pltpu.with_memory_space_constraint(x, pltpu.HBM) for x in operands])


def store_kernel(count, *refs):
    sem = refs[-1]
    copies = [
        pltpu.make_async_copy(refs[i], refs[count + i], sem.at[i]) for i in range(count)
    ]
    for copy in copies:
        copy.start()
    for copy in copies:
        copy.wait()


def store(values):
    count = len(values)
    return pl.pallas_call(
        functools.partial(store_kernel, count),
        out_shape=[jax.ShapeDtypeStruct(v.shape, v.dtype) for v in values],
        in_specs=[pl.BlockSpec(memory_space=pltpu.VMEM)] * count,
        out_specs=[pl.BlockSpec(memory_space=pltpu.HBM)] * count,
        scratch_shapes=[pltpu.SemaphoreType.DMA((count,))],
        compiler_params=pltpu.CompilerParams(vmem_limit_bytes=16 * MIB),
    )(*values)


def local(*args):
    n, nt = lax.axis_size("sp"), lax.axis_size("tp")
    args = args[:2] + (args[2].T, args[3].T) + args[4:]
    gate, up, down, proj, rec, branch = store(fused(args, n, nt))
    return gate[None], up[None], down[None], proj, rec, branch


def solution(mesh):
    placed = (
        P("sp", None),
        P("sp", None),
        P("sp", None),
        P("sp", None),
        P("sp", None, "tp"),
        P("sp", None, "tp"),
        P("sp", "tp", None),
        P(None, "tp"),
        P("tp", "sp"),
        P("tp", "sp"),
        P("tp", "sp"),
        P("tp", "sp"),
        P("tp", None, None),
        P("tp", None, None),
        P("tp"),
        P("tp", "sp"),
    )
    return jax.shard_map(
        local,
        mesh=mesh,
        in_specs=placed,
        out_specs=(
            P("sp", None, "tp"),
            P("sp", None, "tp"),
            P("sp", "tp", None),
            P("sp", "tp"),
            P("tp", "sp"),
            P("tp", "sp"),
        ),
        check_vma=False,
    )
```

```python
import functools

import jax
import jax.numpy as jnp
from jax import lax
from jax.experimental import pallas as pl
from jax.experimental.pallas import tpu as pltpu
from jax.sharding import PartitionSpec as P

RATE_SCALE = 8.0
CLAMP_LIMIT = 7.0
GLU_ALPHA = 1.702
CORES = 2
MESH = pl.DeviceIdType.MESH
MIB = 1024 * 1024
GELU_A = 0.7978845608028654
GELU_B = 0.044715
BF = jnp.bfloat16
F32 = jnp.float32


def aligned(value, size):
    return pl.multiple_of(value * size, size)


def part(index, size):
    return pl.ds(aligned(index, size), size)


def remote(src, dst, send_sem, recv_sem, device):
    return pltpu.make_async_remote_copy(
        src_ref=src,
        dst_ref=dst,
        send_sem=send_sem,
        recv_sem=recv_sem,
        device_id=device,
        device_id_type=MESH,
    )


def dot(a, b, da=1, db=0):
    return lax.dot_general(a, b, (((da,), (db,)), ((), ())), preferred_element_type=F32)


def minus_expm1(x):
    series = x * (1.0 + x * (0.5 + x * (1 / 6 + x * (1 / 24 + x * (1 / 120 + x * (1 / 720))))))
    return jnp.where(x > -0.25, -series, 1.0 - jnp.exp(x))


def softplus(v):
    u = jnp.exp(-jnp.abs(v))
    series = u * (1.0 - u * (0.5 - u * (1 / 3 - u * (0.25 - u * (0.2 - u * (1 / 6))))))
    return jnp.maximum(v, 0.0) + jnp.where(u < 0.06, series, jnp.log(1.0 + u))


def sigmoid(x):
    return 1.0 / (1.0 + jnp.exp(-x))


class Place:
    def __init__(self, n_sp, n_tp):
        self.n, self.nt, self.ny = n_sp, n_tp, n_tp // CORES
        self.s, self.t = lax.axis_index("sp"), lax.axis_index("tp")
        self.y, self.c = self.t // CORES, lax.rem(self.t, CORES)
        self.partner = (self.s, self.y * CORES + 1 - self.c)
        quarter = n_sp // 4
        self.far = (2 * quarter, 3 * quarter)
        self.inner = lax.rem(self.s // quarter + self.s // (2 * quarter), 2) == 1

    def mirror(self, i):
        found, bit = 0, 1
        while bit < self.n:
            found = found + lax.rem(self.s // bit + i // bit, 2) * bit
            bit *= 2
        return found

    def y_peer(self, j):
        return lax.rem(self.y + j, self.ny)

    def y_source(self, j):
        return lax.rem(self.y + self.ny - j, self.ny)

    def tp_of(self, y, c):
        return y * CORES + c

    def q(self, j, same=True):
        return self.tp_of(self.y_source(j), self.c if same else 1 - self.c)

    def y_dev(self, j):
        return (self.s, self.tp_of(self.y_peer(j), self.c))

    def dev(self, i, j):
        return (self.mirror(i), self.tp_of(self.y_peer(j), self.c))


def fused_kernel(n, nt, head_dim, *refs):
    (
        stream_h, cot_h, ids_h, rw_h, wg_h, wu_h, wd_h, op_h, mixed_h, rec_h, branch_h, before_h,
        rgate_h, igate_h, dparam_h, dshift_h,
        st_gate, st_up, st_down, o_proj, o_rec, o_branch,
        wg, wu, wd, opf, sc, pos, land, land2, land_t, src, inb, msrc, mb, act, dg, du, wgp, wup,
        q, qin, qsum, ret, ag, au, gp, gin, gsum, yin, gy, xin, gx, zin, xin2, mx, yin2,
        level, coef, link, links, mixed_t, dm0, adj0, base,
        stream, cot, ids, rw, mixed, rec_in, branch, before, rgate, igate, dparam, dshift,
        w_sem, s1, r1, sy, ry, sx, rx, sm, rm, smy, rmy, smx, rmx, soy, roy, sox, rox,
        sq, rq, sr, rr, sk, rk, sg, rg, sgy, rgy, sgx, rgx, sgz, rgz, sx2, rx2, sy2, ry2,
    ) = refs
    at = Place(n, nt)
    ny = at.ny
    tok, width = cot_h.shape
    rows = land.shape[0] // n
    cols = width // nt
    wl, hidden = opf.shape[2], wg.shape[1]
    top = ids_h.shape[0]
    blk = width // n
    half = n // 2
    quarter = n // 4
    groups = [list(range(nt))] if wl % 128 == 0 else [[b] for b in range(nt)]
    ftile, cross = min(256, hidden), half // 2
    far_1, far_2 = at.far
    near_rows, far_rows = half * rows, quarter * rows
    far_a, far_b = far_1 * rows, far_2 * rows

    def cat(ref, sl, group):
        parts = [ref[b, sl, :] for b in group]
        return parts[0] if len(parts) == 1 else jnp.concatenate(parts, axis=1)

    def spread(value, group, put):
        for at_b, b in enumerate(group):
            put(b, value[:, at_b * wl : (at_b + 1) * wl])

    def settle(ref, sem):
        pltpu.make_async_copy(ref, ref, sem).wait()

    def loop(lo, hi, body):
        def step(i, carry):
            body(i)
            return carry

        lax.fori_loop(lo, hi, step, 0)

    pairs = (
        (ids_h, ids), (rw_h, rw), (stream_h, stream), (cot_h, cot), (op_h, opf.at[at.t]),
        (mixed_h, mixed), (rec_h, rec_in), (branch_h, branch), (before_h, before),
        (rgate_h, rgate), (igate_h, igate), (dparam_h, dparam), (dshift_h, dshift),
        (wg_h, wg), (wu_h, wu), (wd_h, wd),
    )
    loads = [pltpu.make_async_copy(a, b, w_sem.at[i]) for i, (a, b) in enumerate(pairs)]

    for copy in loads:
        copy.start()

    barrier = pltpu.get_barrier_semaphore()

    def greet(device):
        pl.semaphore_signal(barrier, inc=1, device_id=device, device_id_type=MESH)

    def greet_all(i):
        for j in range(ny):
            greet(at.dev(i, j))

    loop(1, n, greet_all)
    for j in range(1, ny):
        greet(at.y_dev(j))
    greet(at.partner)


    lane = lax.broadcasted_iota(jnp.int32, (tok, tok), 1)
    sub = lax.broadcasted_iota(jnp.int32, (tok, tok), 0)
    eye = lane == sub
    eye_low = jnp.where(eye, 1.0, 0.0).astype(BF)
    tri = jnp.where(sub < lane, 1.0, 0.0).astype(BF)
    expert_at = lax.broadcasted_iota(jnp.int32, (n, tok), 0).astype(F32)
    named = []
    loads[0].wait()
    loads[1].wait()
    for k in range(top):
        named.append(expert_at == ids[k : k + 1, :].astype(F32))
    count = functools.reduce(jnp.add, [jnp.where(m, 1.0, 0.0) for m in named])
    earlier = dot(count.astype(BF), tri)
    for k in range(top):
        pos[k] = jnp.where(named[k], earlier, -1.0)
    slot = lax.broadcasted_iota(jnp.int32, (rows, tok), 0).astype(F32)

    def lands(i):
        e = at.mirror(i)
        hits = [jnp.where(pos[k, pl.ds(e, 1), :] == slot, 1.0, 0.0) for k in range(top)]
        land[part(i, rows), :] = functools.reduce(jnp.add, hits).astype(BF)
        for k in range(top):
            land2[part(i, rows), k * tok : (k + 1) * tok] = hits[k].astype(BF)

    loop(0, n, lands)

    share = [
        jnp.sum(jnp.where(eye, rw[k : k + 1, :], 0.0), axis=1, keepdims=True) for k in range(top)
    ]

    def scale(b):
        sl = part(b, cols)
        value = cot[:, sl].astype(F32)
        for k in range(top):
            sc[k * tok : (k + 1) * tok, sl] = (share[k] * value).astype(BF)

    loads[2].wait()
    loads[3].wait()
    loop(0, nt, scale)

    def to_slots(lo, hi, tp, put):
        sl, rs = part(tp, cols), slice(lo * rows, hi * rows)
        put(rs, slice(0, cols), dot(land[rs, :], stream[:, sl]).astype(BF))
        put(rs, slice(cols, 2 * cols), dot(land2[rs, :], sc[:, sl]).astype(BF))

    def put_src(j):
        def put(rs, cs, value):
            src[j, rs, cs] = value

        return put

    for j in range(ny):
        to_slots(1, half, at.q(j), put_src(j))

    def first(i, j, phase=0):
        return remote(
            src.at[j, part(i, rows), :],
            inb.at[at.q(j), part(i, rows), :],
            s1.at[phase],
            r1.at[i],
            (at.mirror(i), at.t),
        )

    def along_y(i, j, outgoing):
        spot = inb.at[at.t if outgoing else at.q(j), part(i, rows), :]
        return remote(spot, spot, sy.at[0], ry.at[i - half, j], at.y_dev(j))

    def across(i, j, group):
        spot = inb.at[at.q(j), part(i, rows), :]
        return remote(spot, spot, sx.at[0], rx.at[group], at.partner)

    def op_y(j, outgoing):
        spot = opf.at[at.t if outgoing else at.q(j)]
        return remote(spot, spot, soy.at[j], roy.at[j], at.y_dev(j))

    def op_x(j, outgoing):
        spot = opf.at[at.q(j, outgoing)]
        return remote(spot, spot, sox.at[j], rox.at[j], at.partner)

    def m_first(i):
        return remote(
            msrc.at[part(i, rows), :],
            mb.at[at.t, part(i, rows), :],
            sm.at[0],
            rm.at[0],
            (at.mirror(i), at.t),
        )

    def m_y(j, outgoing):
        spot = mb.at[at.t if outgoing else at.q(j)]
        return remote(spot, spot, smy.at[j], rmy.at[j], at.y_dev(j))

    def m_x(j, outgoing):
        spot = mb.at[at.q(j, outgoing)]
        return remote(spot, spot, smx.at[j], rmx.at[j], at.partner)

    loads[4].wait()
    loads[5].wait()
    pl.semaphore_wait(barrier, (n - 1) * ny + ny - 1 + 1)
    for j in range(1, ny):
        op_y(j, True).start()
    op_x(0, True).start()

    def send_near(i):
        for j in range(ny):
            first(i, j).start()

    split = half - half // 4
    loop(1, split, send_near)
    to_slots(half, n, at.t, put_src(0))
    msrc[...] = dot(land[...], mixed[...], 1, 1).astype(BF)

    def own_slots(tp):
        def put(rs, cs, value):
            inb[tp, rs, cs] = value

        to_slots(0, 1, tp, put)

    loop(0, nt, own_slots)
    loop(far_1, far_2, lambda i: first(i, 0, 1).start())
    mb[at.t, 0:rows, :] = msrc[0:rows, :]
    loop(split, half, send_near)
    loop(far_2, n, lambda i: first(i, 0, 2).start())
    loop(1, n, lambda i: m_first(i).start())

    lane_w = lax.broadcasted_iota(jnp.int32, (wl, wl), 1)
    sub_w = lax.broadcasted_iota(jnp.int32, (wl, wl), 0)
    eye_w = lane_w == sub_w

    def to_col(row):
        return jnp.sum(jnp.where(eye_w, row, 0.0), axis=1, keepdims=True)

    def to_row(col):
        return jnp.sum(jnp.where(eye_w, col, 0.0), axis=0, keepdims=True)

    repeat = jnp.where(
        lax.rem(lax.broadcasted_iota(jnp.int32, (head_dim, wl), 1), head_dim)
        == lax.broadcasted_iota(jnp.int32, (head_dim, wl), 0),
        1.0,
        0.0,
    ).astype(BF)
    same_head = lax.div(lane_w, head_dim) == lax.div(sub_w, head_dim)

    def diagonal(ref):
        return jnp.where(same_head, dot(ref[...], repeat), 0.0).astype(BF)

    for copy in loads[6:13]:
        copy.wait()
    time_at = lax.broadcasted_iota(jnp.int32, (wl, tok), 1)
    rec = rec_in[...]
    rec_gate = sigmoid(dot(diagonal(rgate), rec, 0, 0))
    in_gate = sigmoid(dot(diagonal(igate), rec, 0, 0))
    rec = rec.astype(F32)
    soft = to_col(softplus(-dparam[...]))
    log_decay = -RATE_SCALE * rec_gate * soft + dshift[...]
    decay = jnp.exp(log_decay)
    at_start = (time_at == 0) & (at.s == 0)
    raw_mult = jnp.sqrt(minus_expm1(2.0 * log_decay))
    multiplier = jnp.where(at_start, 1.0, raw_mult)
    old = before[...]
    state = decay * old + multiplier * in_gate * rec
    x = branch[...].astype(F32)
    th = jnp.tanh(GELU_A * (x + GELU_B * x * x * x))
    gelu = 0.5 * x * (1.0 + th)
    slope = 0.5 * (1.0 + th) + 0.5 * x * (1.0 - th * th) * GELU_A * (1.0 + 3.0 * GELU_B * x * x)
    mult_part = jnp.where(at_start, 0.0, in_gate * rec * decay * decay / raw_mult)
    coef[0] = gelu
    coef[1] = state * slope
    coef[2] = (old * decay - mult_part) * (-RATE_SCALE * soft) * rec_gate * (1.0 - rec_gate)
    coef[3] = multiplier * rec * in_gate * (1.0 - in_gate)
    coef[4] = multiplier * in_gate
    step_decay = jnp.where(time_at == tok - 1, 0.0, pltpu.roll(decay, tok - 1, 1))
    tail = jnp.where(time_at == tok - 1, 1.0, pltpu.roll(decay, tok - 1, 1))
    shift, depth = 1, 0
    while shift < tok:
        level[depth] = step_decay
        step_decay = step_decay * pltpu.roll(step_decay, tok - shift, 1)
        tail = tail * jnp.where(time_at < tok - shift, pltpu.roll(tail, tok - shift, 1), 1.0)
        shift, depth = shift * 2, depth + 1
    coef[5] = tail
    coef[6] = decay
    link[...] = jnp.zeros(link.shape, F32)
    link[0:1, :] = to_row(decay[:, 0:1] * tail[:, 0:1])
    dm0[...] = dot(cot[...], opf[at.t])
    mixed_t[...] = dot(eye_low, mixed[...], 1, 1).astype(BF)
    land_t[...] = dot(eye_low, land[...], 1, 1).astype(BF)

    def own_part(b):
        base[part(b, cols), :] = dot(cot[:, part(b, cols)], mixed_t[...], 0, 0)

    loop(0, nt, own_part)
    for copy in loads[13:]:
        copy.wait()

    def near_in(i):
        settle(src.at[:, 0:rows, :], r1.at[i])
        for j in range(ny):
            across(i, j, 0).start()

    def far_in(group):
        def one(i):
            first(i, 0).wait_recv()
            for j in range(1, ny):
                along_y(i, j, True).start()
            across(i, 0, group).start()

        return one

    def far_pass(group):
        def one(i):
            for j in range(1, ny):
                along_y(i, j, False).wait_recv()
                across(i, j, group).start()

        return one

    def all_here(group, lo, hi):
        settle(inb.at[0:ny, lo * rows : hi * rows, :], rx.at[group])

    def forward(r0, size, lo=0, hi=hidden // ftile):
        rs = pl.ds(r0, size)

        def tile(f):
            fs = part(f, ftile)
            gate = up = d_act = 0.0
            for b in range(nt):
                bs = slice(b * cols, (b + 1) * cols)
                tokens, grads = inb[b, rs, 0:cols], inb[b, rs, cols : 2 * cols]
                gate = gate + dot(tokens, wg[bs, fs])
                up = up + dot(tokens, wu[bs, fs])
                d_act = d_act + dot(grads, wd[fs, bs], 1, 1)
            glu = jnp.minimum(gate, CLAMP_LIMIT)
            lin = jnp.clip(up, -CLAMP_LIMIT, CLAMP_LIMIT) + 1.0
            sig = sigmoid(GLU_ALPHA * glu)
            gs = glu * sig
            act[rs, fs] = (gs * lin).astype(BF)
            curve = lin * (sig + GLU_ALPHA * gs * (1.0 - sig))
            dg[rs, fs] = jnp.where(gate > CLAMP_LIMIT, 0.0, d_act * curve).astype(BF)
            du[rs, fs] = jnp.where(jnp.abs(up) > CLAMP_LIMIT, 0.0, d_act * gs).astype(BF)

        loop(lo, hi, tile)

    def project(r0, size):
        rs = pl.ds(r0, size)
        for group in groups:
            value = dot(dg[rs, :], cat(wgp, slice(None), group))
            value = value + dot(du[rs, :], cat(wup, slice(None), group))

            def put(b, piece):
                q[b, rs, :] = piece.astype(BF)

            spread(value, group, put)

    def q_core(g, r0, size, j, outgoing):
        yj = at.y_peer(j)
        return remote(
            q.at[at.tp_of(yj, 1 - at.c), pl.ds(r0, size), :],
            qin.at[j, pl.ds(r0, size), :],
            sq.at[0],
            rq.at[g, j],
            at.partner,
        )

    def ret_copy(i, j, own=0):
        return remote(
            qsum.at[j, part(i, rows), :],
            ret.at[j, part(i, rows), :],
            sr.at[own],
            rr.at[own],
            at.dev(i, j),
        )

    def q_send(g, r0, size):
        for j in range(ny):
            q_core(g, r0, size, j, True).start()

    def q_reduce(g, r0, size):
        rs = pl.ds(r0, size)
        for j in range(ny):
            q_core(g, r0, size, j, False).wait_recv()
            mine = q[at.tp_of(at.y_peer(j), at.c), rs, :].astype(F32)
            qsum[j, rs, :] = (mine + qin[j, rs, :].astype(F32)).astype(BF)

    def ret_send(i):
        for j in range(ny):
            ret_copy(i, j).start()

    def weight_maps(f):
        fs = part(f, ftile)
        for group in groups:
            for ref, out in ((wg, wgp), (wu, wup)):
                value = 0.0
                for b in range(nt):
                    bs = slice(b * cols, (b + 1) * cols)
                    value = value + dot(ref[bs, fs], cat(opf, bs, group), 0, 0)

                def put(b, piece):
                    out[b, fs, :] = piece.astype(BF)

                spread(value, group, put)

    near_in(1)
    loop(2, split, near_in)
    for j in range(1, ny):
        op_y(j, False).wait_recv()
        op_x(j, True).start()
    loop(far_1, far_2, far_in(1))
    for j in range(ny):
        op_x(j, False).wait_recv()
    loop(0, hidden // ftile, weight_maps)
    loop(far_1, far_2, far_pass(1))
    loop(split, half, near_in)

    @pl.when(at.inner)
    def _():
        loop(far_2, n, far_in(2))

    all_here(0, 1, half)
    forward(0, near_rows)
    project(0, near_rows)
    q_send(0, 0, near_rows)

    @pl.when(jnp.logical_not(at.inner))
    def _():
        loop(far_2, n, far_in(2))

    all_here(1, far_1, far_2)
    settle(msrc.at[rows:, :], rm.at[0])
    for j in range(1, ny):
        m_y(j, True).start()
    m_x(0, True).start()
    forward(far_a, far_rows)
    project(far_a, far_rows)
    q_send(1, far_a, far_rows)
    loop(far_2, n, far_pass(2))
    q_reduce(0, 0, near_rows)
    q_reduce(1, far_a, far_rows)
    ret[0, 0:rows, :] = qsum[0, 0:rows, :]
    for j in range(1, ny):
        ret_copy(0, j, 1).start()
    loop(1, far_2, ret_send)
    all_here(2, far_2, n)
    forward(far_b, far_rows)
    for j in range(1, ny):
        m_y(j, False).wait_recv()
        m_x(j, True).start()
    project(far_b, far_rows)
    q_send(2, far_b, far_rows)
    for j in range(ny):
        m_x(j, False).wait_recv()

    def inner(f):
        fs = part(f, ftile)
        for group in groups:
            right = cat(mb, slice(None), group)
            for ref, out in ((dg, ag), (du, au)):
                value = dot(ref[:, fs], right, 0, 0)

                def put(b, piece):
                    out[b, fs, :] = piece.astype(BF)

                spread(value, group, put)

    loop(0, hidden // ftile, inner)
    q_reduce(2, far_b, far_rows)
    loop(far_2, n, ret_send)

    def g_core(k, j):
        return remote(
            gp.at[k, at.tp_of(at.y_peer(j), 1 - at.c)],
            gin.at[k, j],
            sg.at[0],
            rg.at[k],
            at.partner,
        )

    def outer(k):
        ds = part(at.mirror(k), blk)
        own = base[ds, :]
        for group in groups:
            value = dot(wg[ds, :], cat(ag, slice(None), group))
            value = value + dot(wu[ds, :], cat(au, slice(None), group))

            def put(b, piece):
                gp[k, b] = (piece + jnp.where(at.t == b, own, 0.0)).astype(BF)

            spread(value, group, put)
        for j in range(ny):
            g_core(k, j).start()

    def g_y(k, j):
        return remote(gsum.at[k, j], yin.at[k, j], sgy.at[0], rgy.at[k - half, j], at.y_dev(j))

    def g_x(k):
        h = lax.div(k, 2)
        return remote(gy.at[k], xin.at[h], sgx.at[0], rgx.at[h - cross], (at.mirror(1), at.t))

    def g_z(k):
        return remote(gx.at[k], zin.at[k], sgz.at[0], rgz.at[k], (at.mirror(2 * k), at.t))

    def g_x2(k, j):
        return remote(
            gsum.at[2 * k + 1, j], xin2.at[k, j], sx2.at[0], rx2.at[k], (at.mirror(1), at.t)
        )

    def g_y2(k, j):
        return remote(mx.at[k, j], yin2.at[k, j], sy2.at[0], ry2.at[k, j], at.y_dev(j))

    def core_step(k, y_first):
        settle(gin.at[k], rg.at[k])
        for j in range(ny):
            mine = gp[k, at.tp_of(at.y_peer(j), at.c)].astype(F32)
            gsum[k, j] = (mine + gin[k, j].astype(F32)).astype(BF)
            if y_first:
                if j:
                    g_y(k, j).start()
            else:

                @pl.when(lax.rem(k, 2) == 1)
                def _():
                    g_x2(lax.div(k, 2), j).start()

    def y_step(k):
        total = gsum[k, 0].astype(F32)
        for j in range(1, ny):
            g_y(k, j).wait_recv()
            total = total + yin[k, j].astype(F32)
        gy[k] = total.astype(BF)

    def y_pair(k):
        y_step(2 * k + 1)
        g_x(2 * k + 1).start()
        y_step(2 * k)

    def x_step(k):
        g_x(2 * k + 1).wait_recv()
        gx[k] = (gy[2 * k].astype(F32) + xin[k].astype(F32)).astype(BF)
        g_z(k).start()

    def x2_step(k):
        settle(xin2.at[k], rx2.at[k])
        for j in range(ny):
            both = gsum[2 * k, j].astype(F32) + xin2[k, j].astype(F32)
            mx[k, j] = both.astype(BF)
            if j:
                g_y2(k, j).start()

    def y2_step(k):
        total = mx[k, 0].astype(F32)
        for j in range(1, ny):
            g_y2(k, j).wait_recv()
            total = total + yin2[k, j].astype(F32)
        return total

    def y2_send(k):
        gx[k] = y2_step(k).astype(BF)
        g_z(k).start()

    def wide_tile(d):
        per = cols // min(256, cols)
        size = cols // per
        b, inside = lax.div(d, per), lax.rem(d, per)
        tokens = inb[b, :, part(inside, size)]
        out = part(d, size)
        st_gate[out, :] = dot(tokens, dg[...], 0, 0).astype(BF)
        st_up[out, :] = dot(tokens, du[...], 0, 0).astype(BF)

    def down_tile(f):
        fs = part(f, ftile)
        left = act[:, fs]
        for b in range(nt):
            bs = slice(b * cols, (b + 1) * cols)
            st_down[fs, bs] = dot(left, inb[b, :, cols : 2 * cols], 0, 0).astype(BF)

    outer(n - 1)
    outer(n // 2 - 1)

    def outer_high(i):
        outer(n - 2 - i)
        core_step(n - 1 - i, True)

    def outer_low(i):
        outer(half - 2 - i)
        core_step(half - 1 - i, False)

    def outer_both(i):
        outer_high(i)
        outer_low(i)

    loop(0, half - 1, outer_both)
    core_step(half, True)
    core_step(0, False)

    def tiles(lo, hi):
        count = width // min(256, cols)
        loop(lo * count // 8, hi * count // 8, wide_tile)

    tiles(0, 2)
    y_pair(half - 1)
    x2_step(cross - 1)
    loop(1, half - cross, lambda i: y_pair(half - 1 - i))
    settle(ret.at[:, rows:, :], rr.at[0])
    if ny > 1:
        settle(ret.at[1:, 0:rows, :], rr.at[1])
    total = dm0[...]
    for j in range(ny):
        total = total + dot(land_t[...], ret[j])
    d_mixed = total.T
    o_branch[...] = d_mixed * coef[1]
    run = d_mixed * coef[0]
    shift = 1
    for k in range(depth):
        run = run + level[k] * pltpu.roll(run, tok - shift, 1)
        shift *= 2
    adj0[...] = run
    link[1:2, :] = to_row(coef[6][:, 0:1] * run[:, 0:1])

    def link_copy(i):
        return remote(link, links.at[i], sk.at[0], rk.at[0], (at.mirror(i), at.t))

    loop(1, n, lambda i: link_copy(i).start())
    tiles(2, 4)
    loop(1, cross, lambda i: x2_step(cross - 1 - i))
    x_step(half - 1)
    loop(0, cross - 1, lambda i: y2_send(cross - 1 - i))
    tiles(4, 5)
    loop(1, half - cross, lambda i: x_step(half - 1 - i))
    tiles(5, 8)
    o_proj[...] = y2_step(0)
    loop(0, hidden // ftile, down_tile)
    settle(links.at[1:], rk.at[0])
    links[0] = link[...]

    def compose(k, carry):
        p = n - 1 - k
        lower = links[at.mirror(p)]
        return jnp.where(p > at.s, lower[0:1] * carry + lower[1:2], carry)

    carried = lax.fori_loop(0, n, compose, jnp.zeros((1, wl), F32))
    adjoint = adj0[...] + coef[5] * to_col(carried)
    d_rec = (adjoint * coef[2]).astype(BF)
    d_in = (adjoint * coef[3]).astype(BF)
    o_rec[...] = adjoint * coef[4] + dot(diagonal(rgate), d_rec) + dot(diagonal(igate), d_in)

    def z_step(i):
        k = half - 1 - i
        g_z(k).wait_recv()
        o_proj[...] += zin[k].astype(F32)

    loop(0, half - 1, z_step)

    settle(src.at[:, rows:near_rows, :], s1.at[0])
    settle(src.at[0, far_b:, :], s1.at[2])
    settle(src.at[0, far_a : far_a + far_rows, :], s1.at[1])
    settle(inb.at[0:ny, rows:, :], sx.at[0])
    settle(msrc.at[rows:, :], sm.at[0])
    settle(qin, sq.at[0])
    settle(qsum.at[:, rows:, :], sr.at[0])
    settle(links.at[1:], sk.at[0])
    settle(gin, sg.at[0])
    settle(gx.at[cross:], sgx.at[0])
    settle(zin.at[1:], sgz.at[0])
    settle(xin2, sx2.at[0])
    if ny > 1:
        settle(inb.at[0 : ny - 1, near_rows:, :], sy.at[0])
        settle(qsum.at[1:, 0:rows, :], sr.at[1])
        settle(yin.at[half:, 1:], sgy.at[0])
        settle(yin2.at[:, 1:], sy2.at[0])
    for j in range(1, ny):
        op_y(j, True).wait_send()
        m_y(j, True).wait_send()
    for j in range(ny):
        op_x(j, True).wait_send()
        m_x(j, True).wait_send()


def fused(args, n, nt):
    (stream, cot, ids, rw, wg, wu, wd, op, mixed, rec_in, branch, before, rgate, igate, dparam, dshift) = args
    tok, width = cot.shape
    top = ids.shape[0]
    local_experts, _, hidden = wg.shape
    assert local_experts == 1
    rows = 2 * tok * top // n
    total, ny, cols, wl, blk, half = n * rows, nt // CORES, width // nt, op.shape[1], width // n, n // 2
    head_dim, cross = rgate.shape[1], half // 2
    channels = wl
    dma = pltpu.SemaphoreType.DMA

    def buf(*shape, dtype=BF):
        return pltpu.VMEM(shape, dtype)

    depth = max(1, (tok - 1).bit_length())
    scratch = [
        buf(width, hidden), buf(width, hidden), buf(hidden, width),
        buf(nt, width, wl),
        buf(top * tok, width),
        buf(top, n, tok, dtype=F32),
        buf(total, tok), buf(total, top * tok), buf(tok, total),
        buf(ny, total, 2 * cols), buf(nt, total, 2 * cols),
        buf(total, wl), buf(nt, total, wl),
        buf(total, hidden), buf(total, hidden), buf(total, hidden),
        buf(nt, hidden, wl), buf(nt, hidden, wl),
        buf(nt, total, wl), buf(ny, total, wl), buf(ny, total, wl), buf(ny, total, wl),
        buf(nt, hidden, wl), buf(nt, hidden, wl),
        buf(n, nt, blk, wl), buf(n, ny, blk, wl), buf(n, ny, blk, wl), buf(n, ny, blk, wl),
        buf(n, blk, wl), buf(half, blk, wl), buf(half, blk, wl), buf(half, blk, wl),
        buf(cross, ny, blk, wl), buf(cross, ny, blk, wl), buf(cross, ny, blk, wl),
        buf(depth, wl, tok, dtype=F32), buf(7, wl, tok, dtype=F32),
        buf(8, wl, dtype=F32), buf(n, 8, wl, dtype=F32),
        buf(tok, wl), buf(tok, wl, dtype=F32), buf(wl, tok, dtype=F32), buf(width, wl, dtype=F32),
        buf(tok, width), buf(tok, width), buf(top, tok, dtype=jnp.int32), buf(top, tok, dtype=F32),
        buf(wl, tok), buf(wl, tok), buf(wl, tok), buf(wl, tok, dtype=F32),
        buf(wl, head_dim), buf(wl, head_dim), buf(1, wl, dtype=F32), buf(wl, tok, dtype=F32),
        dma((16,)),
        dma((3,)), dma((n,)), dma((1,)), dma((half, ny)), dma((1,)), dma((3,)),
        dma((1,)), dma((1,)), dma((ny,)), dma((ny,)), dma((ny,)), dma((ny,)),
        dma((ny,)), dma((ny,)), dma((ny,)), dma((ny,)),
        dma((1,)), dma((3, ny)), dma((2,)), dma((2,)), dma((1,)), dma((1,)),
        dma((1,)), dma((n,)), dma((1,)), dma((n - half, ny)),
        dma((1,)), dma((half - cross,)), dma((1,)), dma((half,)),
        dma((1,)), dma((cross,)), dma((1,)), dma((cross, ny)),
    ]
    operands = (
        stream, cot, ids, rw, wg[0], wu[0], wd[0], op, mixed, rec_in, branch, before,
        rgate.reshape(-1, head_dim), igate.reshape(-1, head_dim), dparam[None], dshift,
    )
    kept = 6 * width * hidden + 4 * blk * wl + 8 * wl * tok + MIB
    vm = pl.BlockSpec(memory_space=pltpu.VMEM)
    hb = pl.BlockSpec(memory_space=pltpu.HBM)
    shape = pltpu.VMEM
    return pl.pallas_call(
        functools.partial(fused_kernel, n, nt, head_dim),
        out_shape=(
            shape((width, hidden), BF),
            shape((width, hidden), BF),
            shape((hidden, width), BF),
            shape((blk, wl), F32),
            shape((channels, tok), F32),
            shape((channels, tok), F32),
        ),
        in_specs=[hb] * 16,
        out_specs=[vm] * 6,
        scratch_shapes=scratch,
        compiler_params=pltpu.CompilerParams(
            collective_id=0, has_side_effects=True, vmem_limit_bytes=62 * MIB - kept
        ),
    )(*[pltpu.with_memory_space_constraint(x, pltpu.HBM) for x in operands])


def store_kernel(count, *refs):
    sem = refs[-1]
    copies = [
        pltpu.make_async_copy(refs[i], refs[count + i], sem.at[i]) for i in range(count)
    ]
    for copy in copies:
        copy.start()
    for copy in copies:
        copy.wait()


def store(values):
    count = len(values)
    return pl.pallas_call(
        functools.partial(store_kernel, count),
        out_shape=[jax.ShapeDtypeStruct(v.shape, v.dtype) for v in values],
        in_specs=[pl.BlockSpec(memory_space=pltpu.VMEM)] * count,
        out_specs=[pl.BlockSpec(memory_space=pltpu.HBM)] * count,
        scratch_shapes=[pltpu.SemaphoreType.DMA((count,))],
        compiler_params=pltpu.CompilerParams(vmem_limit_bytes=16 * MIB),
    )(*values)


def local(*args):
    n, nt = lax.axis_size("sp"), lax.axis_size("tp")
    args = args[:2] + (args[2].T, args[3].T) + args[4:]
    gate, up, down, proj, rec, branch = store(fused(args, n, nt))
    return gate[None], up[None], down[None], proj, rec, branch


def solution(mesh):
    placed = (
        P("sp", None),
        P("sp", None),
        P("sp", None),
        P("sp", None),
        P("sp", None, "tp"),
        P("sp", None, "tp"),
        P("sp", "tp", None),
        P(None, "tp"),
        P("tp", "sp"),
        P("tp", "sp"),
        P("tp", "sp"),
        P("tp", "sp"),
        P("tp", None, None),
        P("tp", None, None),
        P("tp"),
        P("tp", "sp"),
    )
    return jax.shard_map(
        local,
        mesh=mesh,
        in_specs=placed,
        out_specs=(
            P("sp", None, "tp"),
            P("sp", None, "tp"),
            P("sp", "tp", None),
            P("sp", "tp"),
            P("tp", "sp"),
            P("tp", "sp"),
        ),
        check_vma=False,
    )
```

```python
import functools

import jax
import jax.numpy as jnp
from jax import lax
from jax.experimental import pallas as pl
from jax.experimental.pallas import tpu as pltpu
from jax.sharding import PartitionSpec as P

RATE_SCALE = 8.0
CLAMP_LIMIT = 7.0
GLU_ALPHA = 1.702
CORES = 2
MESH = pl.DeviceIdType.MESH
MIB = 1024 * 1024
GELU_A = 0.7978845608028654
GELU_B = 0.044715
BF = jnp.bfloat16
F32 = jnp.float32


def aligned(value, size):
    return pl.multiple_of(value * size, size)


def part(index, size):
    return pl.ds(aligned(index, size), size)


def remote(src, dst, send_sem, recv_sem, device):
    return pltpu.make_async_remote_copy(
        src_ref=src,
        dst_ref=dst,
        send_sem=send_sem,
        recv_sem=recv_sem,
        device_id=device,
        device_id_type=MESH,
    )


def dot(a, b, da=1, db=0):
    return lax.dot_general(a, b, (((da,), (db,)), ((), ())), preferred_element_type=F32)


def minus_expm1(x):
    series = x * (1.0 + x * (0.5 + x * (1 / 6 + x * (1 / 24 + x * (1 / 120 + x * (1 / 720))))))
    return jnp.where(x > -0.25, -series, 1.0 - jnp.exp(x))


def softplus(v):
    u = jnp.exp(-jnp.abs(v))
    series = u * (1.0 - u * (0.5 - u * (1 / 3 - u * (0.25 - u * (0.2 - u * (1 / 6))))))
    return jnp.maximum(v, 0.0) + jnp.where(u < 0.06, series, jnp.log(1.0 + u))


def sigmoid(x):
    return 1.0 / (1.0 + jnp.exp(-x))


class Place:
    def __init__(self, n_sp, n_tp):
        self.n, self.nt, self.ny = n_sp, n_tp, n_tp // CORES
        self.s, self.t = lax.axis_index("sp"), lax.axis_index("tp")
        self.y, self.c = self.t // CORES, lax.rem(self.t, CORES)
        self.partner = (self.s, self.y * CORES + 1 - self.c)
        quarter = n_sp // 4
        self.far = (2 * quarter, 3 * quarter)
        self.inner = lax.rem(self.s // quarter + self.s // (2 * quarter), 2) == 1

    def mirror(self, i):
        found, bit = 0, 1
        while bit < self.n:
            found = found + lax.rem(self.s // bit + i // bit, 2) * bit
            bit *= 2
        return found

    def y_peer(self, j):
        return lax.rem(self.y + j, self.ny)

    def y_source(self, j):
        return lax.rem(self.y + self.ny - j, self.ny)

    def tp_of(self, y, c):
        return y * CORES + c

    def q(self, j, same=True):
        return self.tp_of(self.y_source(j), self.c if same else 1 - self.c)

    def y_dev(self, j):
        return (self.s, self.tp_of(self.y_peer(j), self.c))

    def dev(self, i, j):
        return (self.mirror(i), self.tp_of(self.y_peer(j), self.c))


def fused_kernel(n, nt, head_dim, *refs):
    (
        stream_h, cot_h, ids_h, rw_h, wg_h, wu_h, wd_h, op_h, mixed_h, rec_h, branch_h, before_h,
        rgate_h, igate_h, dparam_h, dshift_h,
        st_gate, st_up, st_down, o_proj, o_rec, o_branch,
        wg, wu, wd, opf, sc, pos, land, land2, land_t, src, inb, msrc, mb, act, dg, du, wgp, wup,
        q, qin, qsum, ret, ag, au, gp, gin, gsum, yin, gy, xin, gx, zin, xin2, mx, yin2,
        level, coef, link, links, mixed_t, dm0, adj0, base,
        stream, cot, ids, rw, mixed, rec_in, branch, before, rgate, igate, dparam, dshift,
        w_sem, s1, r1, sy, ry, sx, rx, sm, rm, smy, rmy, smx, rmx, soy, roy, sox, rox,
        sq, rq, sr, rr, sk, rk, sg, rg, sgy, rgy, sgx, rgx, sgz, rgz, sx2, rx2, sy2, ry2,
    ) = refs
    at = Place(n, nt)
    ny = at.ny
    tok, width = cot_h.shape
    rows = land.shape[0] // n
    cols = width // nt
    wl, hidden = opf.shape[2], wg.shape[1]
    top = ids_h.shape[0]
    blk = width // n
    half = n // 2
    quarter = n // 4
    groups = [list(range(nt))] if wl % 128 == 0 else [[b] for b in range(nt)]
    ftile, cross = min(512, hidden), half // 2
    far_1, far_2 = at.far
    near_rows, far_rows = half * rows, quarter * rows
    far_a, far_b = far_1 * rows, far_2 * rows

    def cat(ref, sl, group):
        parts = [ref[b, sl, :] for b in group]
        return parts[0] if len(parts) == 1 else jnp.concatenate(parts, axis=1)

    def spread(value, group, put):
        for at_b, b in enumerate(group):
            put(b, value[:, at_b * wl : (at_b + 1) * wl])

    def settle(ref, sem):
        pltpu.make_async_copy(ref, ref, sem).wait()

    def loop(lo, hi, body):
        def step(i, carry):
            body(i)
            return carry

        lax.fori_loop(lo, hi, step, 0)

    pairs = (
        (ids_h, ids), (rw_h, rw), (stream_h, stream), (cot_h, cot), (op_h, opf.at[at.t]),
        (mixed_h, mixed), (rec_h, rec_in), (branch_h, branch), (before_h, before),
        (rgate_h, rgate), (igate_h, igate), (dparam_h, dparam), (dshift_h, dshift),
        (wg_h, wg), (wu_h, wu), (wd_h, wd),
    )
    loads = [pltpu.make_async_copy(a, b, w_sem.at[i]) for i, (a, b) in enumerate(pairs)]

    for copy in loads:
        copy.start()

    barrier = pltpu.get_barrier_semaphore()

    def greet(device):
        pl.semaphore_signal(barrier, inc=1, device_id=device, device_id_type=MESH)

    def greet_all(i):
        for j in range(ny):
            greet(at.dev(i, j))

    loop(1, n, greet_all)
    for j in range(1, ny):
        greet(at.y_dev(j))
    greet(at.partner)


    lane = lax.broadcasted_iota(jnp.int32, (tok, tok), 1)
    sub = lax.broadcasted_iota(jnp.int32, (tok, tok), 0)
    eye = lane == sub
    eye_low = jnp.where(eye, 1.0, 0.0).astype(BF)
    tri = jnp.where(sub < lane, 1.0, 0.0).astype(BF)
    expert_at = lax.broadcasted_iota(jnp.int32, (n, tok), 0).astype(F32)
    named = []
    loads[0].wait()
    loads[1].wait()
    for k in range(top):
        named.append(expert_at == ids[k : k + 1, :].astype(F32))
    count = functools.reduce(jnp.add, [jnp.where(m, 1.0, 0.0) for m in named])
    earlier = dot(count.astype(BF), tri)
    for k in range(top):
        pos[k] = jnp.where(named[k], earlier, -1.0)
    slot = lax.broadcasted_iota(jnp.int32, (rows, tok), 0).astype(F32)

    def lands(i):
        e = at.mirror(i)
        hits = [jnp.where(pos[k, pl.ds(e, 1), :] == slot, 1.0, 0.0) for k in range(top)]
        land[part(i, rows), :] = functools.reduce(jnp.add, hits).astype(BF)
        for k in range(top):
            land2[part(i, rows), k * tok : (k + 1) * tok] = hits[k].astype(BF)

    loop(0, n, lands)

    share = [
        jnp.sum(jnp.where(eye, rw[k : k + 1, :], 0.0), axis=1, keepdims=True) for k in range(top)
    ]

    def scale(b):
        sl = part(b, cols)
        value = cot[:, sl].astype(F32)
        for k in range(top):
            sc[k * tok : (k + 1) * tok, sl] = (share[k] * value).astype(BF)

    loads[2].wait()
    loads[3].wait()
    loop(0, nt, scale)

    def to_slots(lo, hi, tp, put):
        sl, rs = part(tp, cols), slice(lo * rows, hi * rows)
        put(rs, slice(0, cols), dot(land[rs, :], stream[:, sl]).astype(BF))
        put(rs, slice(cols, 2 * cols), dot(land2[rs, :], sc[:, sl]).astype(BF))

    def put_src(j):
        def put(rs, cs, value):
            src[j, rs, cs] = value

        return put

    for j in range(ny):
        to_slots(1, half, at.q(j), put_src(j))

    def first(i, j, phase=0):
        return remote(
            src.at[j, part(i, rows), :],
            inb.at[at.q(j), part(i, rows), :],
            s1.at[phase],
            r1.at[i],
            (at.mirror(i), at.t),
        )

    def along_y(i, j, outgoing):
        spot = inb.at[at.t if outgoing else at.q(j), part(i, rows), :]
        return remote(spot, spot, sy.at[0], ry.at[i - half, j], at.y_dev(j))

    def across(i, j, group):
        spot = inb.at[at.q(j), part(i, rows), :]
        return remote(spot, spot, sx.at[0], rx.at[group], at.partner)

    def op_y(j, outgoing):
        spot = opf.at[at.t if outgoing else at.q(j)]
        return remote(spot, spot, soy.at[j], roy.at[j], at.y_dev(j))

    def op_x(j, outgoing):
        spot = opf.at[at.q(j, outgoing)]
        return remote(spot, spot, sox.at[j], rox.at[j], at.partner)

    def m_first(i):
        return remote(
            msrc.at[part(i, rows), :],
            mb.at[at.t, part(i, rows), :],
            sm.at[0],
            rm.at[0],
            (at.mirror(i), at.t),
        )

    def m_y(j, outgoing):
        spot = mb.at[at.t if outgoing else at.q(j)]
        return remote(spot, spot, smy.at[j], rmy.at[j], at.y_dev(j))

    def m_x(j, outgoing):
        spot = mb.at[at.q(j, outgoing)]
        return remote(spot, spot, smx.at[j], rmx.at[j], at.partner)

    loads[4].wait()
    loads[5].wait()
    pl.semaphore_wait(barrier, (n - 1) * ny + ny - 1 + 1)
    for j in range(1, ny):
        op_y(j, True).start()
    op_x(0, True).start()

    def send_near(i):
        for j in range(ny):
            first(i, j).start()

    split = half - half // 4
    loop(1, split, send_near)
    to_slots(half, n, at.t, put_src(0))
    msrc[...] = dot(land[...], mixed[...], 1, 1).astype(BF)

    def own_slots(tp):
        def put(rs, cs, value):
            inb[tp, rs, cs] = value

        to_slots(0, 1, tp, put)

    loop(0, nt, own_slots)
    loop(far_1, far_2, lambda i: first(i, 0, 1).start())
    mb[at.t, 0:rows, :] = msrc[0:rows, :]
    loop(split, half, send_near)
    loop(far_2, n, lambda i: first(i, 0, 2).start())
    loop(1, n, lambda i: m_first(i).start())

    lane_w = lax.broadcasted_iota(jnp.int32, (wl, wl), 1)
    sub_w = lax.broadcasted_iota(jnp.int32, (wl, wl), 0)
    eye_w = lane_w == sub_w

    def to_col(row):
        return jnp.sum(jnp.where(eye_w, row, 0.0), axis=1, keepdims=True)

    def to_row(col):
        return jnp.sum(jnp.where(eye_w, col, 0.0), axis=0, keepdims=True)

    repeat = jnp.where(
        lax.rem(lax.broadcasted_iota(jnp.int32, (head_dim, wl), 1), head_dim)
        == lax.broadcasted_iota(jnp.int32, (head_dim, wl), 0),
        1.0,
        0.0,
    ).astype(BF)
    same_head = lax.div(lane_w, head_dim) == lax.div(sub_w, head_dim)

    def diagonal(ref):
        return jnp.where(same_head, dot(ref[...], repeat), 0.0).astype(BF)

    for copy in loads[6:13]:
        copy.wait()
    time_at = lax.broadcasted_iota(jnp.int32, (wl, tok), 1)
    rec = rec_in[...]
    rec_gate = sigmoid(dot(diagonal(rgate), rec, 0, 0))
    in_gate = sigmoid(dot(diagonal(igate), rec, 0, 0))
    rec = rec.astype(F32)
    soft = to_col(softplus(-dparam[...]))
    log_decay = -RATE_SCALE * rec_gate * soft + dshift[...]
    decay = jnp.exp(log_decay)
    at_start = (time_at == 0) & (at.s == 0)
    raw_mult = jnp.sqrt(minus_expm1(2.0 * log_decay))
    multiplier = jnp.where(at_start, 1.0, raw_mult)
    old = before[...]
    state = decay * old + multiplier * in_gate * rec
    x = branch[...].astype(F32)
    th = jnp.tanh(GELU_A * (x + GELU_B * x * x * x))
    gelu = 0.5 * x * (1.0 + th)
    slope = 0.5 * (1.0 + th) + 0.5 * x * (1.0 - th * th) * GELU_A * (1.0 + 3.0 * GELU_B * x * x)
    mult_part = jnp.where(at_start, 0.0, in_gate * rec * decay * decay / raw_mult)
    coef[0] = gelu
    coef[1] = state * slope
    coef[2] = (old * decay - mult_part) * (-RATE_SCALE * soft) * rec_gate * (1.0 - rec_gate)
    coef[3] = multiplier * rec * in_gate * (1.0 - in_gate)
    coef[4] = multiplier * in_gate
    step_decay = jnp.where(time_at == tok - 1, 0.0, pltpu.roll(decay, tok - 1, 1))
    tail = jnp.where(time_at == tok - 1, 1.0, pltpu.roll(decay, tok - 1, 1))
    shift, depth = 1, 0
    while shift < tok:
        level[depth] = step_decay
        step_decay = step_decay * pltpu.roll(step_decay, tok - shift, 1)
        tail = tail * jnp.where(time_at < tok - shift, pltpu.roll(tail, tok - shift, 1), 1.0)
        shift, depth = shift * 2, depth + 1
    coef[5] = tail
    coef[6] = decay
    link[...] = jnp.zeros(link.shape, F32)
    link[0:1, :] = to_row(decay[:, 0:1] * tail[:, 0:1])
    dm0[...] = dot(cot[...], opf[at.t])
    mixed_t[...] = dot(eye_low, mixed[...], 1, 1).astype(BF)
    land_t[...] = dot(eye_low, land[...], 1, 1).astype(BF)

    def own_part(b):
        base[part(b, cols), :] = dot(cot[:, part(b, cols)], mixed_t[...], 0, 0)

    loop(0, nt, own_part)
    for copy in loads[13:]:
        copy.wait()

    def near_in(i):
        settle(src.at[:, 0:rows, :], r1.at[i])
        for j in range(ny):
            across(i, j, 0).start()

    def far_in(group):
        def one(i):
            first(i, 0).wait_recv()
            for j in range(1, ny):
                along_y(i, j, True).start()
            across(i, 0, group).start()

        return one

    def far_pass(group):
        def one(i):
            for j in range(1, ny):
                along_y(i, j, False).wait_recv()
                across(i, j, group).start()

        return one

    def all_here(group, lo, hi):
        settle(inb.at[0:ny, lo * rows : hi * rows, :], rx.at[group])

    def forward(r0, size, lo=0, hi=hidden // ftile):
        rs = pl.ds(r0, size)

        def tile(f):
            fs = part(f, ftile)
            gate = up = d_act = 0.0
            for b in range(nt):
                bs = slice(b * cols, (b + 1) * cols)
                tokens, grads = inb[b, rs, 0:cols], inb[b, rs, cols : 2 * cols]
                gate = gate + dot(tokens, wg[bs, fs])
                up = up + dot(tokens, wu[bs, fs])
                d_act = d_act + dot(grads, wd[fs, bs], 1, 1)
            glu = jnp.minimum(gate, CLAMP_LIMIT)
            lin = jnp.clip(up, -CLAMP_LIMIT, CLAMP_LIMIT) + 1.0
            sig = sigmoid(GLU_ALPHA * glu)
            gs = glu * sig
            act[rs, fs] = (gs * lin).astype(BF)
            curve = lin * (sig + GLU_ALPHA * gs * (1.0 - sig))
            dg[rs, fs] = jnp.where(gate > CLAMP_LIMIT, 0.0, d_act * curve).astype(BF)
            du[rs, fs] = jnp.where(jnp.abs(up) > CLAMP_LIMIT, 0.0, d_act * gs).astype(BF)

        loop(lo, hi, tile)

    def project(r0, size):
        rs = pl.ds(r0, size)
        for group in groups:
            value = dot(dg[rs, :], cat(wgp, slice(None), group))
            value = value + dot(du[rs, :], cat(wup, slice(None), group))

            def put(b, piece):
                q[b, rs, :] = piece.astype(BF)

            spread(value, group, put)

    def q_core(g, r0, size, j, outgoing):
        yj = at.y_peer(j)
        return remote(
            q.at[at.tp_of(yj, 1 - at.c), pl.ds(r0, size), :],
            qin.at[j, pl.ds(r0, size), :],
            sq.at[0],
            rq.at[g, j],
            at.partner,
        )

    def ret_copy(i, j, own=0):
        return remote(
            qsum.at[j, part(i, rows), :],
            ret.at[j, part(i, rows), :],
            sr.at[own],
            rr.at[own],
            at.dev(i, j),
        )

    def q_send(g, r0, size):
        for j in range(ny):
            q_core(g, r0, size, j, True).start()

    def q_reduce(g, r0, size):
        rs = pl.ds(r0, size)
        for j in range(ny):
            q_core(g, r0, size, j, False).wait_recv()
            mine = q[at.tp_of(at.y_peer(j), at.c), rs, :].astype(F32)
            qsum[j, rs, :] = (mine + qin[j, rs, :].astype(F32)).astype(BF)

    def ret_send(i):
        for j in range(ny):
            ret_copy(i, j).start()

    def weight_maps(f):
        fs = part(f, ftile)
        for group in groups:
            for ref, out in ((wg, wgp), (wu, wup)):
                value = 0.0
                for b in range(nt):
                    bs = slice(b * cols, (b + 1) * cols)
                    value = value + dot(ref[bs, fs], cat(opf, bs, group), 0, 0)

                def put(b, piece):
                    out[b, fs, :] = piece.astype(BF)

                spread(value, group, put)

    near_in(1)
    loop(2, split, near_in)
    for j in range(1, ny):
        op_y(j, False).wait_recv()
        op_x(j, True).start()
    loop(far_1, far_2, far_in(1))
    for j in range(ny):
        op_x(j, False).wait_recv()
    loop(0, hidden // ftile, weight_maps)
    loop(far_1, far_2, far_pass(1))
    loop(split, half, near_in)

    @pl.when(at.inner)
    def _():
        loop(far_2, n, far_in(2))

    all_here(0, 1, half)
    forward(0, near_rows)
    project(0, near_rows)
    q_send(0, 0, near_rows)

    @pl.when(jnp.logical_not(at.inner))
    def _():
        loop(far_2, n, far_in(2))

    all_here(1, far_1, far_2)
    settle(msrc.at[rows:, :], rm.at[0])
    for j in range(1, ny):
        m_y(j, True).start()
    m_x(0, True).start()
    forward(far_a, far_rows)
    project(far_a, far_rows)
    q_send(1, far_a, far_rows)
    loop(far_2, n, far_pass(2))
    q_reduce(0, 0, near_rows)
    q_reduce(1, far_a, far_rows)
    ret[0, 0:rows, :] = qsum[0, 0:rows, :]
    for j in range(1, ny):
        ret_copy(0, j, 1).start()
    loop(1, far_2, ret_send)
    all_here(2, far_2, n)
    forward(far_b, far_rows)
    for j in range(1, ny):
        m_y(j, False).wait_recv()
        m_x(j, True).start()
    project(far_b, far_rows)
    q_send(2, far_b, far_rows)
    for j in range(ny):
        m_x(j, False).wait_recv()

    def inner(f):
        fs = part(f, ftile)
        for group in groups:
            right = cat(mb, slice(None), group)
            for ref, out in ((dg, ag), (du, au)):
                value = dot(ref[:, fs], right, 0, 0)

                def put(b, piece):
                    out[b, fs, :] = piece.astype(BF)

                spread(value, group, put)

    loop(0, hidden // ftile, inner)
    q_reduce(2, far_b, far_rows)
    loop(far_2, n, ret_send)

    def g_core(k, j):
        return remote(
            gp.at[k, at.tp_of(at.y_peer(j), 1 - at.c)],
            gin.at[k, j],
            sg.at[0],
            rg.at[k],
            at.partner,
        )

    def outer(k):
        ds = part(at.mirror(k), blk)
        own = base[ds, :]
        for group in groups:
            value = dot(wg[ds, :], cat(ag, slice(None), group))
            value = value + dot(wu[ds, :], cat(au, slice(None), group))

            def put(b, piece):
                gp[k, b] = (piece + jnp.where(at.t == b, own, 0.0)).astype(BF)

            spread(value, group, put)
        for j in range(ny):
            g_core(k, j).start()

    def g_y(k, j):
        return remote(gsum.at[k, j], yin.at[k, j], sgy.at[0], rgy.at[k - half, j], at.y_dev(j))

    def g_x(k):
        h = lax.div(k, 2)
        return remote(gy.at[k], xin.at[h], sgx.at[0], rgx.at[h - cross], (at.mirror(1), at.t))

    def g_z(k):
        return remote(gx.at[k], zin.at[k], sgz.at[0], rgz.at[k], (at.mirror(2 * k), at.t))

    def g_x2(k, j):
        return remote(
            gsum.at[2 * k + 1, j], xin2.at[k, j], sx2.at[0], rx2.at[k], (at.mirror(1), at.t)
        )

    def g_y2(k, j):
        return remote(mx.at[k, j], yin2.at[k, j], sy2.at[0], ry2.at[k, j], at.y_dev(j))

    def core_step(k, y_first):
        settle(gin.at[k], rg.at[k])
        for j in range(ny):
            mine = gp[k, at.tp_of(at.y_peer(j), at.c)].astype(F32)
            gsum[k, j] = (mine + gin[k, j].astype(F32)).astype(BF)
            if y_first:
                if j:
                    g_y(k, j).start()
            else:

                @pl.when(lax.rem(k, 2) == 1)
                def _():
                    g_x2(lax.div(k, 2), j).start()

    def y_step(k):
        total = gsum[k, 0].astype(F32)
        for j in range(1, ny):
            g_y(k, j).wait_recv()
            total = total + yin[k, j].astype(F32)
        gy[k] = total.astype(BF)

    def y_pair(k):
        y_step(2 * k + 1)
        g_x(2 * k + 1).start()
        y_step(2 * k)

    def x_step(k):
        g_x(2 * k + 1).wait_recv()
        gx[k] = (gy[2 * k].astype(F32) + xin[k].astype(F32)).astype(BF)
        g_z(k).start()

    def x2_step(k):
        settle(xin2.at[k], rx2.at[k])
        for j in range(ny):
            both = gsum[2 * k, j].astype(F32) + xin2[k, j].astype(F32)
            mx[k, j] = both.astype(BF)
            if j:
                g_y2(k, j).start()

    def y2_step(k):
        total = mx[k, 0].astype(F32)
        for j in range(1, ny):
            g_y2(k, j).wait_recv()
            total = total + yin2[k, j].astype(F32)
        return total

    def y2_send(k):
        gx[k] = y2_step(k).astype(BF)
        g_z(k).start()

    def wide_tile(d):
        per = cols // min(256, cols)
        size = cols // per
        b, inside = lax.div(d, per), lax.rem(d, per)
        tokens = inb[b, :, part(inside, size)]
        out = part(d, size)
        st_gate[out, :] = dot(tokens, dg[...], 0, 0).astype(BF)
        st_up[out, :] = dot(tokens, du[...], 0, 0).astype(BF)

    def down_tile(f):
        fs = part(f, ftile)
        left = act[:, fs]
        for b in range(nt):
            bs = slice(b * cols, (b + 1) * cols)
            st_down[fs, bs] = dot(left, inb[b, :, cols : 2 * cols], 0, 0).astype(BF)

    outer(n - 1)
    outer(n // 2 - 1)

    def outer_high(i):
        outer(n - 2 - i)
        core_step(n - 1 - i, True)

    def outer_low(i):
        outer(half - 2 - i)
        core_step(half - 1 - i, False)

    def outer_both(i):
        outer_high(i)
        outer_low(i)

    loop(0, half - 1, outer_both)
    core_step(half, True)
    core_step(0, False)

    def tiles(lo, hi):
        count = width // min(256, cols)
        loop(lo * count // 8, hi * count // 8, wide_tile)

    tiles(0, 2)
    y_pair(half - 1)
    x2_step(cross - 1)
    loop(1, half - cross, lambda i: y_pair(half - 1 - i))
    settle(ret.at[:, rows:, :], rr.at[0])
    if ny > 1:
        settle(ret.at[1:, 0:rows, :], rr.at[1])
    total = dm0[...]
    for j in range(ny):
        total = total + dot(land_t[...], ret[j])
    d_mixed = total.T
    o_branch[...] = d_mixed * coef[1]
    run = d_mixed * coef[0]
    shift = 1
    for k in range(depth):
        run = run + level[k] * pltpu.roll(run, tok - shift, 1)
        shift *= 2
    adj0[...] = run
    link[1:2, :] = to_row(coef[6][:, 0:1] * run[:, 0:1])

    def link_copy(i):
        return remote(link, links.at[i], sk.at[0], rk.at[0], (at.mirror(i), at.t))

    loop(1, n, lambda i: link_copy(i).start())
    tiles(2, 4)
    loop(1, cross, lambda i: x2_step(cross - 1 - i))
    x_step(half - 1)
    loop(0, cross - 1, lambda i: y2_send(cross - 1 - i))
    tiles(4, 5)
    loop(1, half - cross, lambda i: x_step(half - 1 - i))
    tiles(5, 8)
    o_proj[...] = y2_step(0)
    loop(0, hidden // ftile, down_tile)
    settle(links.at[1:], rk.at[0])
    links[0] = link[...]

    def compose(k, carry):
        p = n - 1 - k
        lower = links[at.mirror(p)]
        return jnp.where(p > at.s, lower[0:1] * carry + lower[1:2], carry)

    carried = lax.fori_loop(0, n, compose, jnp.zeros((1, wl), F32))
    adjoint = adj0[...] + coef[5] * to_col(carried)
    d_rec = (adjoint * coef[2]).astype(BF)
    d_in = (adjoint * coef[3]).astype(BF)
    o_rec[...] = adjoint * coef[4] + dot(diagonal(rgate), d_rec) + dot(diagonal(igate), d_in)

    def z_step(i):
        k = half - 1 - i
        g_z(k).wait_recv()
        o_proj[...] += zin[k].astype(F32)

    loop(0, half - 1, z_step)

    settle(src.at[:, rows:near_rows, :], s1.at[0])
    settle(src.at[0, far_b:, :], s1.at[2])
    settle(src.at[0, far_a : far_a + far_rows, :], s1.at[1])
    settle(inb.at[0:ny, rows:, :], sx.at[0])
    settle(msrc.at[rows:, :], sm.at[0])
    settle(qin, sq.at[0])
    settle(qsum.at[:, rows:, :], sr.at[0])
    settle(links.at[1:], sk.at[0])
    settle(gin, sg.at[0])
    settle(gx.at[cross:], sgx.at[0])
    settle(zin.at[1:], sgz.at[0])
    settle(xin2, sx2.at[0])
    if ny > 1:
        settle(inb.at[0 : ny - 1, near_rows:, :], sy.at[0])
        settle(qsum.at[1:, 0:rows, :], sr.at[1])
        settle(yin.at[half:, 1:], sgy.at[0])
        settle(yin2.at[:, 1:], sy2.at[0])
    for j in range(1, ny):
        op_y(j, True).wait_send()
        m_y(j, True).wait_send()
    for j in range(ny):
        op_x(j, True).wait_send()
        m_x(j, True).wait_send()


def fused(args, n, nt):
    (stream, cot, ids, rw, wg, wu, wd, op, mixed, rec_in, branch, before, rgate, igate, dparam, dshift) = args
    tok, width = cot.shape
    top = ids.shape[0]
    local_experts, _, hidden = wg.shape
    assert local_experts == 1
    rows = 2 * tok * top // n
    total, ny, cols, wl, blk, half = n * rows, nt // CORES, width // nt, op.shape[1], width // n, n // 2
    head_dim, cross = rgate.shape[1], half // 2
    channels = wl
    dma = pltpu.SemaphoreType.DMA

    def buf(*shape, dtype=BF):
        return pltpu.VMEM(shape, dtype)

    depth = max(1, (tok - 1).bit_length())
    scratch = [
        buf(width, hidden), buf(width, hidden), buf(hidden, width),
        buf(nt, width, wl),
        buf(top * tok, width),
        buf(top, n, tok, dtype=F32),
        buf(total, tok), buf(total, top * tok), buf(tok, total),
        buf(ny, total, 2 * cols), buf(nt, total, 2 * cols),
        buf(total, wl), buf(nt, total, wl),
        buf(total, hidden), buf(total, hidden), buf(total, hidden),
        buf(nt, hidden, wl), buf(nt, hidden, wl),
        buf(nt, total, wl), buf(ny, total, wl), buf(ny, total, wl), buf(ny, total, wl),
        buf(nt, hidden, wl), buf(nt, hidden, wl),
        buf(n, nt, blk, wl), buf(n, ny, blk, wl), buf(n, ny, blk, wl), buf(n, ny, blk, wl),
        buf(n, blk, wl), buf(half, blk, wl), buf(half, blk, wl), buf(half, blk, wl),
        buf(cross, ny, blk, wl), buf(cross, ny, blk, wl), buf(cross, ny, blk, wl),
        buf(depth, wl, tok, dtype=F32), buf(7, wl, tok, dtype=F32),
        buf(8, wl, dtype=F32), buf(n, 8, wl, dtype=F32),
        buf(tok, wl), buf(tok, wl, dtype=F32), buf(wl, tok, dtype=F32), buf(width, wl, dtype=F32),
        buf(tok, width), buf(tok, width), buf(top, tok, dtype=jnp.int32), buf(top, tok, dtype=F32),
        buf(wl, tok), buf(wl, tok), buf(wl, tok), buf(wl, tok, dtype=F32),
        buf(wl, head_dim), buf(wl, head_dim), buf(1, wl, dtype=F32), buf(wl, tok, dtype=F32),
        dma((16,)),
        dma((3,)), dma((n,)), dma((1,)), dma((half, ny)), dma((1,)), dma((3,)),
        dma((1,)), dma((1,)), dma((ny,)), dma((ny,)), dma((ny,)), dma((ny,)),
        dma((ny,)), dma((ny,)), dma((ny,)), dma((ny,)),
        dma((1,)), dma((3, ny)), dma((2,)), dma((2,)), dma((1,)), dma((1,)),
        dma((1,)), dma((n,)), dma((1,)), dma((n - half, ny)),
        dma((1,)), dma((half - cross,)), dma((1,)), dma((half,)),
        dma((1,)), dma((cross,)), dma((1,)), dma((cross, ny)),
    ]
    operands = (
        stream, cot, ids, rw, wg[0], wu[0], wd[0], op, mixed, rec_in, branch, before,
        rgate.reshape(-1, head_dim), igate.reshape(-1, head_dim), dparam[None], dshift,
    )
    kept = 6 * width * hidden + 4 * blk * wl + 8 * wl * tok + MIB
    vm = pl.BlockSpec(memory_space=pltpu.VMEM)
    hb = pl.BlockSpec(memory_space=pltpu.HBM)
    shape = pltpu.VMEM
    return pl.pallas_call(
        functools.partial(fused_kernel, n, nt, head_dim),
        out_shape=(
            shape((width, hidden), BF),
            shape((width, hidden), BF),
            shape((hidden, width), BF),
            shape((blk, wl), F32),
            shape((channels, tok), F32),
            shape((channels, tok), F32),
        ),
        in_specs=[hb] * 16,
        out_specs=[vm] * 6,
        scratch_shapes=scratch,
        compiler_params=pltpu.CompilerParams(
            collective_id=0, has_side_effects=True, vmem_limit_bytes=62 * MIB - kept
        ),
    )(*[pltpu.with_memory_space_constraint(x, pltpu.HBM) for x in operands])


def store_kernel(count, *refs):
    sem = refs[-1]
    copies = [
        pltpu.make_async_copy(refs[i], refs[count + i], sem.at[i]) for i in range(count)
    ]
    for copy in copies:
        copy.start()
    for copy in copies:
        copy.wait()


def store(values):
    count = len(values)
    return pl.pallas_call(
        functools.partial(store_kernel, count),
        out_shape=[jax.ShapeDtypeStruct(v.shape, v.dtype) for v in values],
        in_specs=[pl.BlockSpec(memory_space=pltpu.VMEM)] * count,
        out_specs=[pl.BlockSpec(memory_space=pltpu.HBM)] * count,
        scratch_shapes=[pltpu.SemaphoreType.DMA((count,))],
        compiler_params=pltpu.CompilerParams(vmem_limit_bytes=16 * MIB),
    )(*values)


def local(*args):
    n, nt = lax.axis_size("sp"), lax.axis_size("tp")
    args = args[:2] + (args[2].T, args[3].T) + args[4:]
    gate, up, down, proj, rec, branch = store(fused(args, n, nt))
    return gate[None], up[None], down[None], proj, rec, branch


def solution(mesh):
    placed = (
        P("sp", None),
        P("sp", None),
        P("sp", None),
        P("sp", None),
        P("sp", None, "tp"),
        P("sp", None, "tp"),
        P("sp", "tp", None),
        P(None, "tp"),
        P("tp", "sp"),
        P("tp", "sp"),
        P("tp", "sp"),
        P("tp", "sp"),
        P("tp", None, None),
        P("tp", None, None),
        P("tp"),
        P("tp", "sp"),
    )
    return jax.shard_map(
        local,
        mesh=mesh,
        in_specs=placed,
        out_specs=(
            P("sp", None, "tp"),
            P("sp", None, "tp"),
            P("sp", "tp", None),
            P("sp", "tp"),
            P("tp", "sp"),
            P("tp", "sp"),
        ),
        check_vma=False,
    )
```
